32 devices in a mesh: sp: 16 (over z, y, x), tp: 2 (over core).
Axes of the slice: x: 2, y: 2, z: 4, core: 2. Of those that a mesh axis runs over, the one named last changes fastest.
Arguments:
- residual_in: bfloat16 [4096, 2048], P('sp'), may hold values from -6 to 6
- mixer_input: bfloat16 [2048, 4096], P('tp', 'sp'), may hold values from -6 to 6
- branch_gate: bfloat16 [2048, 4096], P('tp', 'sp'), may hold values from -6 to 6
- conv_taps: bfloat16 [2048, 4], P('tp'), may hold values from -3 to 3
- recur_weight: bfloat16 [32, 64, 64], P('tp'), may hold values from -0.75 to 0.75
- admit_weight: bfloat16 [32, 64, 64], P('tp'), may hold values from -0.75 to 0.75
- decay_param: float32 [2048], P('tp'), may hold values from 4 to 16
- decay_extra: float32 [2048, 4096], P('tp', 'sp'), may hold values from -1 to 0
- out_weight: bfloat16 [2048, 2048], P('tp'), may hold values from -0.375 to 0.375
- norm_gain: bfloat16 [2048], replicated, may hold values from 0.099609375 to 1.8984375
- gate_weight: bfloat16 [2048, 5632], P('sp', 'tp'), may hold values from -0.125 to 0.125
- up_weight: bfloat16 [2048, 5632], P('sp', 'tp'), may hold values from -0.125 to 0.125
- down_weight: bfloat16 [2048, 5632], P('sp', 'tp'), may hold values from -0.15625 to 0.15625
Outputs:
- layer_out: bfloat16 [4096, 2048], P('sp')
The draws below stay inside these ranges and needn't reach their ends.
All inputs are finite; a program needn't handle non-finite values.
Results may differ from the reference program's by a relative error of at most 0.019.
Values may be sent and summed in bfloat16 or wider, within the bound.
A program may use at most 128 MiB of HBM per device.

```python
import jax
import jax.numpy as jnp
from jax import lax

D = 2048
W = 2048
BLOCKS = 32
BLOCK = 64
FF = 5632
KERNEL = 4
TOK_DEV = 256
TOKENS = 4096
N_SP = 16
N_TP = 2


def draw_decay_param(key, part):
    pick_key, slow_key, fast_key = jax.random.split(key, 3)
    slow_share = 0.5
    slow_rate = jax.random.uniform(slow_key, (W,), jnp.float32, 0.2, 0.6) / (4.0 * TOKENS)
    fast_rate = jnp.exp(jax.random.uniform(fast_key, (W,), jnp.float32, jnp.log(0.0025), jnp.log(0.01)))
    chosen = jax.random.uniform(pick_key, (W,), jnp.float32) < slow_share
    picked_rate = jnp.where(chosen, slow_rate, fast_rate)
    return (-jnp.log(jnp.expm1(picked_rate))).astype(jnp.float32)


def draw_decay_extra(key, part):
    level_key, spot_key, loss_key = jax.random.split(key, 3)
    low_end = 0.15
    high_end = 0.9
    block_count = TOKENS // TOK_DEV
    levels = jnp.exp(jax.random.uniform(level_key, (W, block_count), jnp.float32, jnp.log(low_end), jnp.log(high_end))) / TOKENS
    steady = -jnp.repeat(levels, TOK_DEV, axis=1)
    spots = jax.random.randint(spot_key, (3,), 0, TOKENS)
    losses = jnp.log1p(-jax.random.uniform(loss_key, (W, 3), jnp.float32, 0.2, 0.4))
    positions = jnp.arange(TOKENS)
    result_field = steady
    for which in range(3):
        hit_row = (positions == spots[which]).astype(jnp.float32)
        result_field = result_field + losses[:, which:which + 1] * hit_row[None, :]
    return result_field.astype(jnp.float32)


def shard_levels(key, shape, cuts, smallest, largest):
    loudness = 1.0
    for position, shards_of in cuts:
        steps = jax.random.uniform(jax.random.fold_in(jax.random.fold_in(key, 6), position), (shards_of,), jnp.float32, smallest / len(cuts), largest / len(cuts))
        loudness = loudness * jnp.repeat(jnp.exp(steps), shape[position] // shards_of).reshape((-1,) + (1,) * (len(shape) - 1 - position))
    return loudness


def normal_values(stream_key, shape, deviation, most, pieces=(), held_as=jnp.bfloat16):
    factor_of = shard_levels(stream_key, shape, pieces, -0.22, 0.18) if pieces else 1.0
    drawn = jax.random.normal(stream_key, shape, jnp.float32) * deviation * factor_of
    return jnp.minimum(jnp.maximum(drawn, -most), most).astype(held_as)


def setup_inputs(seed: int = 0) -> dict:
    keys = jax.random.split(jax.random.key(seed), 14)
    return {
        "residual_in": normal_values(keys[0], (TOKENS, D), 1.0, 6.0, ((0, 16),)),
        "mixer_input": normal_values(keys[1], (W, TOKENS), 1.0, 6.0, ((0, 2), (1, 16))),
        "branch_gate": normal_values(keys[2], (W, TOKENS), 1.0, 6.0, ((0, 2), (1, 16))),
        "conv_taps": normal_values(keys[3], (W, KERNEL), KERNEL ** -0.5, 3.0, ((0, 2),)),
        "recur_weight": normal_values(keys[4], (BLOCKS, BLOCK, BLOCK), BLOCK ** -0.5, 0.75, ((0, 2),)),
        "admit_weight": normal_values(keys[5], (BLOCKS, BLOCK, BLOCK), BLOCK ** -0.5, 0.75, ((0, 2),)),
        "decay_param": draw_decay_param(jax.random.fold_in(keys[13], 71), 0),
        "decay_extra": draw_decay_extra(jax.random.fold_in(keys[13], 71), 0),
        "out_weight": normal_values(keys[8], (W, D), (W // 8) ** -0.5, 0.375, ((0, 2),)),
        "norm_gain": jnp.clip(1.0 + 0.18 * jax.random.normal(keys[9], (D,), jnp.float32), 0.099609375, 1.8984375).astype(jnp.bfloat16),
        "gate_weight": normal_values(keys[10], (D, FF), D ** -0.5, 0.125, ((0, 16), (1, 2))),
        "up_weight": normal_values(keys[11], (D, FF), D ** -0.5, 0.125, ((0, 16), (1, 2))),
        "down_weight": normal_values(keys[12], (D, FF), (FF // 4) ** -0.5, 0.15625, ((0, 16), (1, 2))),
    }


def block_gates(weight, signal):
    groups = weight.shape[0]
    grouped = signal.astype(jnp.float32).reshape(groups, weight.shape[1], signal.shape[1])
    mapped = jnp.einsum('gij,git->gjt', weight.astype(jnp.float32), grouped)
    return jax.nn.sigmoid(mapped.reshape(signal.shape))

def link_pairs(earlier, latter):
    return (earlier[0] * latter[0], latter[0] * earlier[1] + latter[1])

def reference(residual_in, mixer_input, branch_gate, conv_taps, recur_weight, admit_weight, decay_param, decay_extra, out_weight, norm_gain, gate_weight, up_weight, down_weight):
    tap_count = conv_taps.shape[1]
    length = mixer_input.shape[1]
    padded = jnp.pad(mixer_input.astype(jnp.float32), ((0, 0), (tap_count - 1, 0)))
    tap_values = conv_taps.astype(jnp.float32)
    conv_sum = jnp.zeros(mixer_input.shape, jnp.float32)
    for tap in range(tap_count):
        conv_sum = conv_sum + tap_values[:, tap:tap + 1] * padded[:, tap:tap + length]
    conv_out = conv_sum.astype(jnp.bfloat16)
    recur_gate = block_gates(recur_weight, conv_out)
    admit_gate = block_gates(admit_weight, conv_out)
    base_rate = jax.nn.softplus(-decay_param.astype(jnp.float32))[:, None]
    log_decay = -8.0 * recur_gate * base_rate + decay_extra
    decay_step = jnp.exp(log_decay)
    drive_term = jnp.sqrt(-jnp.expm1(2.0 * log_decay)) * admit_gate * conv_out.astype(jnp.float32)
    running, states = lax.associative_scan(link_pairs, (decay_step, drive_term), axis=1)
    gate_act = jax.nn.gelu(branch_gate.astype(jnp.float32), approximate=True)
    mixed_out = (states * gate_act).astype(jnp.bfloat16)
    model_width = residual_in.shape[1]
    split_width = gate_weight.shape[1] // N_TP
    res_blocks = residual_in.reshape(N_SP, TOK_DEV, model_width)
    mix_blocks = mixed_out.reshape(mixed_out.shape[0], N_SP, TOK_DEV).transpose(1, 0, 2)
    gain_wide = norm_gain.astype(jnp.float32)
    down_split = down_weight.astype(jnp.float32).reshape(model_width, N_TP, split_width)

    def one_block(pair):
        resid, mix_block = pair
        branch = jnp.dot(mix_block.T, out_weight, preferred_element_type=jnp.float32)
        middle = (resid.astype(jnp.float32) + branch).astype(jnp.bfloat16)
        middle_wide = middle.astype(jnp.float32)
        row_scale = lax.rsqrt(lax.optimization_barrier(jnp.mean(middle_wide * middle_wide, axis=1, keepdims=True)) + 1e-06)
        normed = (middle_wide * row_scale * gain_wide).astype(jnp.bfloat16)
        gate_pre = jnp.dot(normed, gate_weight, preferred_element_type=jnp.float32)
        up_pre = jnp.dot(normed, up_weight, preferred_element_type=jnp.float32)
        hidden = (jax.nn.silu(gate_pre) * up_pre).astype(jnp.bfloat16)
        hidden_split = hidden.astype(jnp.float32).reshape(hidden.shape[0], N_TP, split_width)
        partial_value = jnp.einsum('tkf,dkf->ktd', hidden_split, down_split).astype(jnp.bfloat16)
        partial_value = lax.optimization_barrier(partial_value)
        channel_out = lax.optimization_barrier(jnp.sum(partial_value.astype(jnp.float32), axis=0))
        return (middle.astype(jnp.float32) + channel_out).astype(jnp.bfloat16)
    layer_blocks = lax.map(one_block, (res_blocks, mix_blocks))
    return layer_blocks.reshape(N_SP * TOK_DEV, model_width)
```

```python
import functools

import jax
import jax.numpy as jnp
from jax import lax
from jax.experimental import pallas as pl
from jax.experimental.pallas import tpu as pltpu
from jax.sharding import PartitionSpec as P

MESH = pl.DeviceIdType.MESH
LANES = 128


def neg_expm1(v):
    series = jnp.full_like(v, 1.0)
    for k in range(9, 1, -1):
        series = 1.0 + series * v * (1.0 / k)
    return jnp.where(v > -0.5, -v * series, 1.0 - jnp.exp(v))


def mixer_kernel(
    n,
    x_ref,
    halo_ref,
    bg_ref,
    extra_ref,
    taps_ref,
    rate_ref,
    wr_ref,
    wa_ref,
    out_ref,
    state_s,
    run_s,
    ends_s,
    all_s,
    in_s,
    send_sem,
    recv_sem,
):
    me = lax.axis_index("sp")
    barrier = pltpu.get_barrier_semaphore()

    def greet(k, carry):
        pl.semaphore_signal(
            barrier, inc=1, device_id={"sp": lax.rem(me + k, n)}, device_id_type=MESH
        )
        return carry

    lax.fori_loop(1, n, greet, 0)
    channels, length = x_ref.shape
    block = wr_ref.shape[1]
    groups = channels // LANES
    tap_count = taps_ref.shape[1]
    lane = lax.broadcasted_iota(jnp.int32, (LANES, length), 1)

    def local(g, carry):
        rows = pl.ds(pl.multiple_of(g * LANES, LANES), LANES)
        wide = jnp.concatenate(
            [halo_ref[rows, :].astype(jnp.float32), x_ref[rows, :].astype(jnp.float32)], axis=1
        )
        taps = taps_ref[rows, :]
        total = taps[:, tap_count - 1 :] * wide[:, LANES:]
        for tap in range(tap_count - 2, -1, -1):
            total = total + taps[:, tap : tap + 1] * pltpu.roll(wide, tap_count - 1 - tap, 1)[:, LANES:]
        conv = total.astype(jnp.bfloat16)
        per = LANES // block
        recur, admit = [], []
        for b in range(per):
            part = conv[b * block : (b + 1) * block]
            recur.append(jnp.dot(wr_ref[g * per + b], part, preferred_element_type=jnp.float32))
            admit.append(jnp.dot(wa_ref[g * per + b], part, preferred_element_type=jnp.float32))
        recur = jax.nn.sigmoid(jnp.concatenate(recur, axis=0))
        admit = jax.nn.sigmoid(jnp.concatenate(admit, axis=0))
        log_decay = recur * rate_ref[rows, :] + extra_ref[rows, :]
        a = jnp.exp(log_decay)
        b = jnp.sqrt(neg_expm1(2.0 * log_decay)) * admit * conv.astype(jnp.float32)
        shift = 1
        while shift < length:
            seen = lane >= shift
            b = b + a * jnp.where(seen, pltpu.roll(b, shift, 1), 0.0)
            a = a * jnp.where(seen, pltpu.roll(a, shift, 1), 1.0)
            shift *= 2
        state_s[rows, :] = b
        run_s[rows, :] = a
        ends_s[pl.ds(g, 1), :] = a[:, length - LANES :].T[LANES - 1 :]
        ends_s[pl.ds(groups + g, 1), :] = b[:, length - LANES :].T[LANES - 1 :]
        return carry

    lax.fori_loop(0, groups, local, 0)
    pl.semaphore_wait(barrier, n - 1)

    def copy_to(k):
        return pltpu.make_async_remote_copy(
            src_ref=ends_s,
            dst_ref=all_s.at[k - 1],
            send_sem=send_sem.at[k - 1],
            recv_sem=recv_sem.at[k - 1],
            device_id={"sp": lax.rem(me + k, n)},
            device_id_type=MESH,
        )

    def send(k, carry):
        copy_to(k).start()
        return carry

    lax.fori_loop(1, n, send, 0)

    def finish(k, carry):
        copy_to(k).wait()
        return carry

    lax.fori_loop(1, n, finish, 0)

    def fold(i, before):
        k = n - 1 - i
        part = all_s[k - 1]
        new = part[:groups] * before + part[groups:]
        return jnp.where(k <= me, new, before)

    in_s[...] = lax.fori_loop(0, n - 1, fold, jnp.zeros((groups, LANES), jnp.float32))

    def close(g, carry):
        rows = pl.ds(pl.multiple_of(g * LANES, LANES), LANES)
        entering = jnp.broadcast_to(in_s[pl.ds(g, 1), :], (LANES, LANES)).T
        entering = jnp.concatenate([entering] * (length // LANES), axis=1)
        states = state_s[rows, :] + run_s[rows, :] * entering
        v = bg_ref[rows, :].astype(jnp.float32)
        act = 0.5 * v * (1.0 + jnp.tanh(0.7978845608028654 * (v + 0.044715 * v * v * v)))
        out_ref[rows, :] = (states * act).astype(jnp.bfloat16)
        return carry

    lax.fori_loop(0, groups, close, 0)


def mixer(n, x, halo, bg, extra, taps, rate, wr, wa):
    channels, length = x.shape
    groups = channels // LANES
    vmem = pl.BlockSpec(memory_space=pltpu.VMEM)
    return pl.pallas_call(
        functools.partial(mixer_kernel, n),
        out_shape=jax.ShapeDtypeStruct((channels, length), jnp.bfloat16),
        in_specs=[vmem] * 8,
        out_specs=vmem,
        scratch_shapes=[
            pltpu.VMEM((channels, length), jnp.float32),
            pltpu.VMEM((channels, length), jnp.float32),
            pltpu.VMEM((2 * groups, LANES), jnp.float32),
            pltpu.VMEM((n - 1, 2 * groups, LANES), jnp.float32),
            pltpu.VMEM((groups, LANES), jnp.float32),
            pltpu.SemaphoreType.DMA((n - 1,)),
            pltpu.SemaphoreType.DMA((n - 1,)),
        ],
        compiler_params=pltpu.CompilerParams(
            collective_id=0, has_side_effects=True, vmem_limit_bytes=24 << 20
        ),
        cost_estimate=pl.CostEstimate(
            flops=200 * channels * length, bytes_accessed=12 * channels * length, transcendentals=0
        ),
        name="mixer",
    )(x, halo, bg, extra, taps, rate, wr, wa)


def layer_kernel(
    n, split,
    x_ref, bg_ref, extra_ref, taps_ref, dp_ref, wr_ref, wa_ref, ow_ref, res_ref, gain_ref,
    gw_ref, uw_ref, dw_ref,
    out_ref,
    x_s, bg_s, extra_s, ow_s, res_s, raw_s, pack_s,
    xt_s, halo_s, wbd_s, a_s, b_s, ea_s, eb_s, act_s, ends_s, all_s, in_s, mix_s,
    part_s, part_r, mid_s, tok_s, wide_s, hid_s, ff_s, tp_s, red_s, rz_s,
    in_sem, hs_sem, hr_sem, ss_sem, sr_sem,
    zs_sem, zr_sem, ps_sem, pr_sem, fs_sem, fr_sem, rs_sem, rr_sem,
    bs_sem, br_sem, ts_sem, tr_sem, cs_sem, cr_sem,
    as_sem, ar_sem, ks_sem, kr_sem, os_sem, or_sem,
):
    me = lax.axis_index("sp")
    core = lax.axis_index("tp")
    plane = n // split
    rank, spot = me // plane, lax.rem(me, plane)
    f32, bf16 = jnp.float32, jnp.bfloat16
    channels, length = x_s.shape
    groups = channels // LANES
    block = wr_ref.shape[1]
    taps = taps_ref.shape[0]
    kinds, full, depth = pack_s.shape
    span = full // split
    width = mid_s.shape[1]
    barrier = pltpu.get_barrier_semaphore()

    raw_refs = (gw_ref, uw_ref, dw_ref)
    loads = [
        pltpu.make_async_copy(src, dst, in_sem.at[i])
        for i, (src, dst) in enumerate(
            [
                (x_ref, x_s),
                (gw_ref, raw_s.at[0]),
                (uw_ref, raw_s.at[1]),
                (dw_ref, raw_s.at[2]),
                (extra_ref, extra_s),
                (bg_ref, bg_s),
                (ow_ref, ow_s),
                (res_ref, res_s),
            ]
        )
    ]
    for load in loads:
        load.start()

    def greet(k, carry):
        pl.semaphore_signal(
            barrier, inc=1, device_id={"sp": lax.rem(me + k, n)}, device_id_type=MESH
        )
        return carry

    lax.fori_loop(1, n, greet, 0)
    pl.semaphore_signal(barrier, inc=1, device_id={"tp": 1 - core}, device_id_type=MESH)

    def remote(src, dst, ssem, rsem, where):
        return pltpu.make_async_remote_copy(
            src_ref=src, dst_ref=dst, send_sem=ssem, recv_sem=rsem,
            device_id=where, device_id_type=MESH,
        )

    def lanes(i):
        return pl.ds(pl.multiple_of(i * LANES, LANES), LANES)

    def own(c):
        return pack_s.at[c, pl.ds(pl.multiple_of(rank * span, span), span)]

    def window(c, source):
        return wide_s.at[c, :, lanes(source)]

    def z_copy(c, k):
        to = lax.rem(rank + k, split)
        return remote(
            pack_s.at[c, pl.ds(pl.multiple_of(to * span, span), span)], window(c, me),
            zs_sem.at[c, k - 1], zr_sem.at[c, k - 1], {"sp": to * plane + spot},
        )

    def from_rank(k):
        return lax.rem(rank - k + split, split)

    def z_landed(c, k):
        source = from_rank(k) * plane + spot
        return remote(
            own(c), window(c, source), zs_sem.at[c, k - 1], zr_sem.at[c, k - 1], {"sp": source}
        )

    def beside(m):
        return spot + 1 - 2 * lax.rem(spot, 2) if m == 1 else spot + 2 - 4 * (spot // 2)

    def pass_copy(c, k, m):
        source = from_rank(k) * plane + spot
        return remote(
            window(c, source) if k else own(c), window(c, source),
            fs_sem.at[c, k, m - 1], fr_sem.at[c, k, m - 1], {"sp": rank * plane + beside(m)},
        )

    def pass_landed(c, k, m):
        source = from_rank(k) * plane + beside(m)
        return remote(
            window(c, source), window(c, source),
            fs_sem.at[c, k, m - 1], fr_sem.at[c, k, m - 1], {"sp": rank * plane + beside(m)},
        )

    def relay_window(c, k, m, where):
        source = from_rank(k) * plane + where
        return wide_s.at[c, pl.ds((m - 1) * (span // 2), span // 2), lanes(source)]

    def relay_copy(c, k, m):
        view = relay_window(c, k, m, beside(m))
        return remote(
            view, view, rs_sem.at[c, k, m - 1], rr_sem.at[c, k, m - 1],
            {"sp": rank * plane + beside(3 - m)},
        )

    def relay_landed(c, k, m):
        view = relay_window(c, k, m, 3 - spot)
        return remote(
            view, view, rs_sem.at[c, k, m - 1], rr_sem.at[c, k, m - 1],
            {"sp": rank * plane + beside(3 - m)},
        )

    def z_start(c):
        for k in range(1, split):
            z_copy(c, k).start()

    def spread(c, k):
        if k:
            z_landed(c, k).wait_recv()
        for m in (1, 2):
            pass_copy(c, k, m).start()

    def relay(c, k):
        for m in (1, 2):
            pass_landed(c, k, m).wait_recv()
            relay_copy(c, k, m).start()

    def settle(c):
        for k in range(split):
            for m in (1, 2):
                relay_landed(c, k, m).wait_recv()

    def turn(c):
        loads[1 + c].wait()

        def step(j, carry):
            pack_s[c, lanes(j), :] = raw_s[c, :, lanes(j)].T
            return carry

        lax.fori_loop(0, full // LANES, step, 0)

    def keep(c):
        wide_s[c, :, lanes(me)] = own(c)[...]

    loads[0].wait()

    def flip(g, carry):
        xt_s[pl.ds(8, length), lanes(g)] = x_s[lanes(g), :].astype(f32).T
        return carry

    lax.fori_loop(0, groups, flip, 0)
    turn(0)
    pl.semaphore_wait(barrier, n)
    halo = remote(
        xt_s.at[pl.ds(length, 8), :], halo_s, hs_sem, hr_sem, {"sp": lax.rem(me + 1, n)}
    )
    halo.start()
    z_start(0)
    spread(0, 0)
    turn(1)
    spread(1, 0)
    turn(2)
    spread(2, 0)
    for c in range(kinds):
        keep(c)

    rowb = lax.broadcasted_iota(jnp.int32, (LANES, LANES), 0) // block
    colb = lax.broadcasted_iota(jnp.int32, (LANES, LANES), 1) // block
    eye_r = lax.broadcasted_iota(jnp.int32, (block, LANES), 0)
    eye_c = lax.rem(lax.broadcasted_iota(jnp.int32, (block, LANES), 1), block)
    twice = jnp.where(eye_r == eye_c, 1.0, 0.0).astype(bf16)

    def widen(g, carry):
        for slot, w_ref in ((0, wr_ref), (1, wa_ref)):
            pair = jnp.concatenate([w_ref[2 * g], w_ref[2 * g + 1]], axis=0)
            both = jnp.dot(pair, twice, preferred_element_type=f32)
            wbd_s[g, :, slot * LANES : (slot + 1) * LANES] = jnp.where(
                rowb == colb, both, 0.0
            ).astype(bf16)
        return carry

    lax.fori_loop(0, groups, widen, 0)
    loads[4].wait()
    halo.wait()
    xt_s[0:8, :] = halo_s[...] * jnp.where(me > 0, 1.0, 0.0)

    octets = length // 8
    sub = lax.broadcasted_iota(jnp.int32, (octets, 8, LANES), 1)
    row = lax.broadcasted_iota(jnp.int32, (octets, LANES), 0)

    def local(g, carry):
        cols = lanes(g)
        tap = taps_ref[:, cols].astype(f32)
        total = tap[taps - 1 : taps] * xt_s[pl.ds(8, length), cols]
        for k in range(taps - 2, -1, -1):
            total = total + tap[k : k + 1] * xt_s[pl.ds(9 - taps + k, length), cols]
        conv = total.astype(bf16)
        both = jnp.dot(conv, wbd_s[g], preferred_element_type=f32)
        recur = jax.nn.sigmoid(both[:, :LANES])
        admit = jax.nn.sigmoid(both[:, LANES:])
        rate = -8.0 * jax.nn.softplus(-dp_ref[pl.ds(g, 1), :])
        log_decay = recur * rate + extra_s[lanes(g), :].T
        a = jnp.exp(log_decay)
        b = jnp.sqrt(neg_expm1(2.0 * log_decay)) * admit * conv.astype(f32)
        a = a.reshape(octets, 8, LANES)
        b = b.reshape(octets, 8, LANES)
        for shift in (1, 2, 4):
            seen = sub >= shift
            b = b + a * jnp.where(seen, pltpu.roll(b, shift, 1), 0.0)
            a = a * jnp.where(seen, pltpu.roll(a, shift, 1), 1.0)
        a_s[g] = a.reshape(length, LANES)
        b_s[g] = b.reshape(length, LANES)
        ea = a_s[g, pl.ds(7, octets, stride=8), :]
        eb = b_s[g, pl.ds(7, octets, stride=8), :]
        shift = 1
        while shift < octets:
            seen = row >= shift
            eb = eb + ea * jnp.where(seen, pltpu.roll(eb, shift, 0), 0.0)
            ea = ea * jnp.where(seen, pltpu.roll(ea, shift, 0), 1.0)
            shift *= 2
        ends_s[pl.ds(g, 1), :] = ea[octets - 1 :]
        ends_s[pl.ds(groups + g, 1), :] = eb[octets - 1 :]
        ea_s[g] = jnp.where(row >= 1, pltpu.roll(ea, 1, 0), 1.0)
        eb_s[g] = jnp.where(row >= 1, pltpu.roll(eb, 1, 0), 0.0)
        return carry

    lax.fori_loop(0, groups, local, 0)

    def state(k):
        return remote(
            ends_s, all_s.at[k - 1], ss_sem.at[k - 1], sr_sem.at[k - 1],
            {"sp": lax.rem(me + k, n)},
        )

    def state_send(k, carry):
        state(k).start()
        return carry

    lax.fori_loop(1, n, state_send, 0)
    for c in range(kinds):
        relay(c, 0)
    for k in range(1, split):
        spread(0, k)
    z_start(1)
    loads[5].wait()

    def gelu(g, carry):
        v = bg_s[lanes(g), :].astype(f32).T
        act_s[g] = 0.5 * v * (1.0 + jnp.tanh(0.7978845608028654 * (v + 0.044715 * v * v * v)))
        return carry

    lax.fori_loop(0, groups, gelu, 0)

    def state_wait(k, carry):
        state(k).wait()
        return carry

    lax.fori_loop(1, n, state_wait, 0)

    def fold(i, before):
        k = n - 1 - i
        part = all_s[k - 1]
        new = part[:groups] * before + part[groups:]
        return jnp.where(k <= me, new, before)

    in_s[...] = lax.fori_loop(0, n - 1, fold, jnp.zeros((groups, LANES), f32))

    def close(g, carry):
        enter = eb_s[g] + ea_s[g] * in_s[pl.ds(g, 1), :]
        states = jnp.concatenate(
            [
                b_s[g, i * 8 : i * 8 + 8, :] + a_s[g, i * 8 : i * 8 + 8, :] * enter[i : i + 1]
                for i in range(octets)
            ],
            axis=0,
        )
        mix_s[:, lanes(g)] = (states * act_s[g]).astype(bf16)
        return carry

    lax.fori_loop(0, groups, close, 0)

    pieces, row_count, cut = part_s.shape

    def swap(i):
        return remote(
            part_s.at[i], part_r.at[i], bs_sem.at[i], br_sem.at[i], {"tp": 1 - core}
        )

    loads[6].wait()
    for i in range(pieces):
        part_s[i] = jnp.dot(
            mix_s[...], ow_s[:, i * cut : (i + 1) * cut], preferred_element_type=f32
        ).astype(bf16)
        swap(i).start()
    for k in range(1, split):
        relay(0, k)
    loads[7].wait()
    square = jnp.zeros((row_count, 1), f32)
    for i in range(pieces):
        swap(i).wait()
        cols = slice(i * cut, (i + 1) * cut)
        branch = part_s[i].astype(f32) + part_r[i].astype(f32)
        middle = (res_s[:, cols].astype(f32) + branch).astype(bf16)
        mid_s[:, cols] = middle
        middle = middle.astype(f32)
        square = square + jnp.sum(middle * middle, axis=1, keepdims=True)
    scale = lax.rsqrt(square * (1.0 / (pieces * cut)) + 1e-06)
    for i in range(width // LANES):
        cols = slice(i * LANES, (i + 1) * LANES)
        gain = gain_ref[i : i + 1, :].astype(f32)
        tok_s[rank, :, cols] = (mid_s[:, cols].astype(f32) * scale * gain).astype(bf16)

    half = row_count // 2
    mine = pl.ds(pl.multiple_of(core * half, half), half)
    other = pl.ds(pl.multiple_of((1 - core) * half, half), half)

    def tok_copy(way, d):
        step = 1 - 2 * way
        view = tok_s.at[rank - (d - 1) * step, mine, :]
        return remote(
            view, view, ts_sem.at[way, d - 1], tr_sem.at[way, d - 1],
            {"sp": (rank + step) * plane + spot},
        )

    def tok_landed(way, d):
        step = 1 - 2 * way
        view = tok_s.at[rank - d * step, mine, :]
        return remote(
            view, view, ts_sem.at[way, d - 1], tr_sem.at[way, d - 1],
            {"sp": (rank - step) * plane + spot},
        )

    def tok_pass(way, d, rows):
        view = tok_s.at[rank - d * (1 - 2 * way), rows, :]
        return remote(
            view, view, cs_sem.at[way, d - 1], cr_sem.at[way, d - 1], {"tp": 1 - core}
        )

    def held(way, d):
        return rank >= d if way == 0 else rank <= split - 1 - d

    def onward(way, d):
        return (
            jnp.logical_and(rank >= d, rank < split - 1)
            if way == 0
            else jnp.logical_and(rank <= split - 1 - d, rank > 0)
        )

    for way in (0, 1):

        @pl.when(onward(way, 0))
        def _():
            tok_copy(way, 1).start()

    def tok_relay(d):
        for way in (0, 1):

            @pl.when(held(way, d))
            def _():
                tok_landed(way, d).wait_recv()
                tok_pass(way, d, mine).start()

            if d < split - 1:

                @pl.when(onward(way, d))
                def _():
                    tok_copy(way, d + 1).start()

    def tok_ready(d):
        for way in (0, 1):

            @pl.when(held(way, d))
            def _():
                tok_pass(way, d, other).wait_recv()

    z_start(2)
    for k in range(1, split):
        spread(1, k)
    for k in range(1, split):
        relay(1, k)
    tok_relay(1)
    settle(0)
    settle(1)
    for k in range(1, split):
        spread(2, k)
    tok_relay(2)
    for k in range(1, split):
        relay(2, k)
    tok_relay(3)
    settle(2)
    for d in range(1, split):
        tok_ready(d)

    side = rank // 2
    inner = lax.rem(rank, 2) + side - 2 * lax.rem(rank, 2) * side
    chunks, _, chunk = ff_s.shape[1:]
    across = (((1,), (1,)), ((), ()))

    def target(i):
        t = (3, 2, 1 - inner, inner)[i]
        return t + side * (split - 1 - 2 * t)

    def feed(i):
        tokens = tok_s[target(i)]
        gate = lax.dot_general(tokens, wide_s[0], across, preferred_element_type=f32)
        up = lax.dot_general(tokens, wide_s[1], across, preferred_element_type=f32)
        hid_s[...] = (gate / (1.0 + jnp.exp(-gate)) * up).astype(bf16)
        for q in range(chunks):
            ff_s[i, q] = jnp.dot(
                hid_s[...], wide_s[2, :, q * chunk : (q + 1) * chunk], preferred_element_type=f32
            ).astype(bf16)
            tp_copy(i, q).start()

    def tp_copy(i, q):
        return remote(
            ff_s.at[i, q, other, :], tp_s.at[i, q], as_sem.at[i, q], ar_sem.at[i, q],
            {"tp": 1 - core},
        )

    mate = rank + 1 - 2 * lax.rem(rank, 2)
    ahead = rank + 1 - 2 * side

    def sum_copy(i, q):
        slot = i + 3 * inner if i < 2 else 2 + inner
        to = ahead if i < 2 else mate
        return remote(
            red_s.at[i, q], rz_s.at[slot, q], ks_sem.at[i, q], kr_sem.at[slot, q],
            {"sp": to * plane + spot},
        )

    def sum_landed(slot, q):
        return remote(
            red_s.at[0, q], rz_s.at[slot, q], ks_sem.at[0, q], kr_sem.at[slot, q],
            {"sp": mate * plane + spot},
        )

    def pair(i, q):
        tp_copy(i, q).wait()
        return ff_s[i, q, mine, :].astype(f32) + tp_s[i, q].astype(f32)

    def push(i, q):
        slot = i if i < 2 else 3

        @pl.when(inner == 0)
        def _():
            red_s[i, q] = pair(i, q).astype(bf16)

        @pl.when(inner == 1)
        def _():
            mixed = pair(i, q)
            sum_landed(slot, q).wait_recv()
            red_s[i, q] = (mixed + rz_s[slot, q].astype(f32)).astype(bf16)

        sum_copy(i, q).start()

    def out_copy(q):
        view = out_ref.at[mine, pl.ds(q * chunk, chunk)]
        return remote(view, view, os_sem.at[q], or_sem.at[q], {"tp": 1 - core})

    def out_landed(q):
        view = out_ref.at[other, pl.ds(q * chunk, chunk)]
        return remote(view, view, os_sem.at[q], or_sem.at[q], {"tp": 1 - core})

    def finish(q):
        cols = slice(q * chunk, (q + 1) * chunk)
        i = split - 1
        base = mid_s[mine, cols].astype(f32)

        @pl.when(inner == 0)
        def _():
            mixed = pair(i, q)
            sum_landed(3, q).wait_recv()
            out_ref[mine, cols] = (base + (mixed + rz_s[3, q].astype(f32))).astype(bf16)

        @pl.when(inner == 1)
        def _():
            mixed = pair(i, q)
            sum_landed(2, q).wait_recv()
            mixed = mixed + rz_s[2, q].astype(f32)
            sum_landed(4, q).wait_recv()
            out_ref[mine, cols] = (base + (mixed + rz_s[4, q].astype(f32))).astype(bf16)

        out_copy(q).start()

    feed(0)
    feed(1)
    for q in range(chunks):
        push(0, q)
    feed(2)
    for q in range(chunks):
        push(1, q)
    feed(3)
    for q in range(chunks):
        push(2, q)
    for q in range(chunks):
        finish(q)

    for q in range(chunks):
        out_copy(q).wait_send()
        out_landed(q).wait_recv()
        for i in range(split - 1):
            sum_copy(i, q).wait_send()
    for way in (0, 1):
        for d in range(1, split):

            @pl.when(onward(way, d - 1))
            def _():
                tok_copy(way, d).wait_send()

            @pl.when(held(way, d))
            def _():
                tok_pass(way, d, mine).wait_send()

    for c in range(kinds):
        for k in range(split):
            for m in (1, 2):
                pass_copy(c, k, m).wait_send()
                relay_copy(c, k, m).wait_send()
            if k:
                z_copy(c, k).wait_send()


def layer(n, split, x, bg, extra, taps, dp, wr, wa, ow, res, gain, gw, uw, dw):
    channels, length = x.shape
    groups = channels // LANES
    rows, width = res.shape
    depth, full = gw.shape
    span = full // split
    kinds = 3
    cut = 512
    pieces = width // cut
    chunk = width // 2
    chunks = width // chunk
    half = rows // 2
    vmem = pl.BlockSpec(memory_space=pltpu.VMEM)
    hbm = pl.BlockSpec(memory_space=pl.ANY)
    dma = pltpu.SemaphoreType.DMA
    bf16, f32 = jnp.bfloat16, jnp.float32
    buf = pltpu.VMEM
    return pl.pallas_call(
        functools.partial(layer_kernel, n, split),
        out_shape=jax.ShapeDtypeStruct((rows, width), bf16),
        in_specs=[hbm, hbm, hbm, vmem, vmem, vmem, vmem, hbm, hbm, vmem, hbm, hbm, hbm],
        out_specs=vmem,
        scratch_shapes=[
            buf((channels, length), bf16),
            buf((channels, length), bf16),
            buf((channels, length), f32),
            buf((channels, width), bf16),
            buf((rows, width), bf16),
            buf((kinds, depth, full), bf16),
            buf((kinds, full, depth), bf16),
            buf((length + 8, channels), f32),
            buf((8, channels), f32),
            buf((groups, LANES, 2 * LANES), bf16),
            buf((groups, length, LANES), f32),
            buf((groups, length, LANES), f32),
            buf((groups, length // 8, LANES), f32),
            buf((groups, length // 8, LANES), f32),
            buf((groups, length, LANES), f32),
            buf((2 * groups, LANES), f32),
            buf((n - 1, 2 * groups, LANES), f32),
            buf((groups, LANES), f32),
            buf((length, channels), bf16),
            buf((pieces, rows, cut), bf16),
            buf((pieces, rows, cut), bf16),
            buf((rows, width), bf16),
            buf((split, rows, width), bf16),
            buf((kinds, span, width), bf16),
            buf((rows, span), bf16),
            buf((split, chunks, rows, chunk), bf16),
            buf((split, chunks, half, chunk), bf16),
            buf((split - 1, chunks, half, chunk), bf16),
            buf((5, chunks, half, chunk), bf16),
            dma((8,)),
            dma,
            dma,
            dma((n - 1,)),
            dma((n - 1,)),
            dma((kinds, split - 1)),
            dma((kinds, split - 1)),
            dma((1,)),
            dma((1,)),
            dma((kinds, split, 2)),
            dma((kinds, split, 2)),
            dma((kinds, split, 2)),
            dma((kinds, split, 2)),
            dma((pieces,)),
            dma((pieces,)),
            dma((2, split - 1)),
            dma((2, split - 1)),
            dma((2, split - 1)),
            dma((2, split - 1)),
            dma((split, chunks)),
            dma((split, chunks)),
            dma((split - 1, chunks)),
            dma((5, chunks)),
            dma((chunks,)),
            dma((chunks,)),
        ],
        compiler_params=pltpu.CompilerParams(
            collective_id=1, has_side_effects=True, vmem_limit_bytes=60 << 20
        ),
        name="layer",
    )(x, bg, extra, taps, dp, wr, wa, ow, res, gain, gw, uw, dw)


def on_device(
    residual_in,
    mixer_input,
    branch_gate,
    conv_taps,
    recur_weight,
    admit_weight,
    decay_param,
    decay_extra,
    out_weight,
    norm_gain,
    gate_weight,
    up_weight,
    down_weight,
):
    n = lax.axis_size("sp")
    length = mixer_input.shape[1]
    width, share_ff = residual_in.shape[1], gate_weight.shape[1]
    split = 4
    depth = gate_weight.shape[0]
    if (
        lax.axis_size("tp") == 2
        and n == 4 * split
        and depth == LANES
        and width == n * depth
        and share_ff % LANES == 0
        and share_ff % (32 * split) == 0
        and 2 * recur_weight.shape[1] == LANES
        and conv_taps.shape[1] <= 9
        and residual_in.shape[0] == length
        and length % (2 * LANES) == 0
    ):
        return layer(
            n,
            split,
            mixer_input,
            branch_gate,
            decay_extra,
            conv_taps.T,
            decay_param.reshape(-1, LANES),
            recur_weight,
            admit_weight,
            out_weight,
            residual_in,
            norm_gain.reshape(-1, LANES),
            gate_weight,
            up_weight,
            down_weight,
        )
    halo = lax.ppermute(
        mixer_input[:, length - LANES :], "sp", [(i, i + 1) for i in range(n - 1)]
    )
    rate = -8.0 * jax.nn.softplus(-decay_param)[:, None]
    mixed_out = mixer(
        n,
        mixer_input,
        halo,
        branch_gate,
        decay_extra,
        conv_taps.astype(jnp.float32),
        rate,
        recur_weight.transpose(0, 2, 1),
        admit_weight.transpose(0, 2, 1),
    )
    row_count = residual_in.shape[0]
    partial_value = lax.dot_general(
        mixed_out, out_weight, (((0,), (0,)), ((), ())), preferred_element_type=jnp.float32
    )
    branch = lax.psum(partial_value.astype(jnp.bfloat16), "tp").astype(jnp.float32)
    middle = (residual_in.astype(jnp.float32) + branch).astype(jnp.bfloat16)
    middle_wide = middle.astype(jnp.float32)
    row_scale = lax.rsqrt(jnp.mean(middle_wide * middle_wide, axis=1, keepdims=True) + 1e-06)
    normed = (middle_wide * row_scale * norm_gain.astype(jnp.float32)).astype(jnp.bfloat16)
    gate_pre = jnp.dot(
        normed,
        lax.all_gather(gate_weight, "sp", axis=0, tiled=True),
        preferred_element_type=jnp.float32,
    )
    up_pre = jnp.dot(
        normed,
        lax.all_gather(up_weight, "sp", axis=0, tiled=True),
        preferred_element_type=jnp.float32,
    )
    down_whole = lax.all_gather(down_weight, "sp", axis=0, tiled=True)
    hidden = (jax.nn.silu(gate_pre) * up_pre).astype(jnp.bfloat16)
    share = row_count // lax.axis_size("tp")
    channel_out = lax.psum_scatter(
        lax.dot_general(
            hidden, down_whole, (((1,), (1,)), ((), ())), preferred_element_type=jnp.float32
        ).astype(jnp.bfloat16),
        "tp",
        scatter_dimension=0,
        tiled=True,
    ).astype(jnp.float32)
    first_row = lax.axis_index("tp") * share
    own_rows = lax.dynamic_slice_in_dim(middle, first_row, share, 0)
    layer_rows = (own_rows.astype(jnp.float32) + channel_out).astype(jnp.bfloat16)
    return lax.all_gather(layer_rows, "tp", axis=0, tiled=True)


def solution(mesh):
    placed = (
        P("sp", None),
        P("tp", "sp"),
        P("tp", "sp"),
        P("tp", None),
        P("tp", None, None),
        P("tp", None, None),
        P("tp"),
        P("tp", "sp"),
        P("tp", None),
        P(),
        P("sp", "tp"),
        P("sp", "tp"),
        P("sp", "tp"),
    )
    return jax.shard_map(
        on_device, mesh=mesh, in_specs=placed, out_specs=P("sp", None), check_vma=False
    )
```

```python
import functools

import jax
import jax.numpy as jnp
from jax import lax
from jax.experimental import pallas as pl
from jax.experimental.pallas import tpu as pltpu
from jax.sharding import PartitionSpec as P

MESH = pl.DeviceIdType.MESH
LANES = 128


def neg_expm1(v):
    series = jnp.full_like(v, 1.0)
    for k in range(9, 1, -1):
        series = 1.0 + series * v * (1.0 / k)
    return jnp.where(v > -0.5, -v * series, 1.0 - jnp.exp(v))


def mixer_kernel(
    n,
    x_ref,
    halo_ref,
    bg_ref,
    extra_ref,
    taps_ref,
    rate_ref,
    wr_ref,
    wa_ref,
    out_ref,
    state_s,
    run_s,
    ends_s,
    all_s,
    in_s,
    send_sem,
    recv_sem,
):
    me = lax.axis_index("sp")
    barrier = pltpu.get_barrier_semaphore()

    def greet(k, carry):
        pl.semaphore_signal(
            barrier, inc=1, device_id={"sp": lax.rem(me + k, n)}, device_id_type=MESH
        )
        return carry

    lax.fori_loop(1, n, greet, 0)
    channels, length = x_ref.shape
    block = wr_ref.shape[1]
    groups = channels // LANES
    tap_count = taps_ref.shape[1]
    lane = lax.broadcasted_iota(jnp.int32, (LANES, length), 1)

    def local(g, carry):
        rows = pl.ds(pl.multiple_of(g * LANES, LANES), LANES)
        wide = jnp.concatenate(
            [halo_ref[rows, :].astype(jnp.float32), x_ref[rows, :].astype(jnp.float32)], axis=1
        )
        taps = taps_ref[rows, :]
        total = taps[:, tap_count - 1 :] * wide[:, LANES:]
        for tap in range(tap_count - 2, -1, -1):
            total = total + taps[:, tap : tap + 1] * pltpu.roll(wide, tap_count - 1 - tap, 1)[:, LANES:]
        conv = total.astype(jnp.bfloat16)
        per = LANES // block
        recur, admit = [], []
        for b in range(per):
            part = conv[b * block : (b + 1) * block]
            recur.append(jnp.dot(wr_ref[g * per + b], part, preferred_element_type=jnp.float32))
            admit.append(jnp.dot(wa_ref[g * per + b], part, preferred_element_type=jnp.float32))
        recur = jax.nn.sigmoid(jnp.concatenate(recur, axis=0))
        admit = jax.nn.sigmoid(jnp.concatenate(admit, axis=0))
        log_decay = recur * rate_ref[rows, :] + extra_ref[rows, :]
        a = jnp.exp(log_decay)
        b = jnp.sqrt(neg_expm1(2.0 * log_decay)) * admit * conv.astype(jnp.float32)
        shift = 1
        while shift < length:
            seen = lane >= shift
            b = b + a * jnp.where(seen, pltpu.roll(b, shift, 1), 0.0)
            a = a * jnp.where(seen, pltpu.roll(a, shift, 1), 1.0)
            shift *= 2
        state_s[rows, :] = b
        run_s[rows, :] = a
        ends_s[pl.ds(g, 1), :] = a[:, length - LANES :].T[LANES - 1 :]
        ends_s[pl.ds(groups + g, 1), :] = b[:, length - LANES :].T[LANES - 1 :]
        return carry

    lax.fori_loop(0, groups, local, 0)
    pl.semaphore_wait(barrier, n - 1)

    def copy_to(k):
        return pltpu.make_async_remote_copy(
            src_ref=ends_s,
            dst_ref=all_s.at[k - 1],
            send_sem=send_sem.at[k - 1],
            recv_sem=recv_sem.at[k - 1],
            device_id={"sp": lax.rem(me + k, n)},
            device_id_type=MESH,
        )

    def send(k, carry):
        copy_to(k).start()
        return carry

    lax.fori_loop(1, n, send, 0)

    def finish(k, carry):
        copy_to(k).wait()
        return carry

    lax.fori_loop(1, n, finish, 0)

    def fold(i, before):
        k = n - 1 - i
        part = all_s[k - 1]
        new = part[:groups] * before + part[groups:]
        return jnp.where(k <= me, new, before)

    in_s[...] = lax.fori_loop(0, n - 1, fold, jnp.zeros((groups, LANES), jnp.float32))

    def close(g, carry):
        rows = pl.ds(pl.multiple_of(g * LANES, LANES), LANES)
        entering = jnp.broadcast_to(in_s[pl.ds(g, 1), :], (LANES, LANES)).T
        entering = jnp.concatenate([entering] * (length // LANES), axis=1)
        states = state_s[rows, :] + run_s[rows, :] * entering
        v = bg_ref[rows, :].astype(jnp.float32)
        act = 0.5 * v * (1.0 + jnp.tanh(0.7978845608028654 * (v + 0.044715 * v * v * v)))
        out_ref[rows, :] = (states * act).astype(jnp.bfloat16)
        return carry

    lax.fori_loop(0, groups, close, 0)


def mixer(n, x, halo, bg, extra, taps, rate, wr, wa):
    channels, length = x.shape
    groups = channels // LANES
    vmem = pl.BlockSpec(memory_space=pltpu.VMEM)
    return pl.pallas_call(
        functools.partial(mixer_kernel, n),
        out_shape=jax.ShapeDtypeStruct((channels, length), jnp.bfloat16),
        in_specs=[vmem] * 8,
        out_specs=vmem,
        scratch_shapes=[
            pltpu.VMEM((channels, length), jnp.float32),
            pltpu.VMEM((channels, length), jnp.float32),
            pltpu.VMEM((2 * groups, LANES), jnp.float32),
            pltpu.VMEM((n - 1, 2 * groups, LANES), jnp.float32),
            pltpu.VMEM((groups, LANES), jnp.float32),
            pltpu.SemaphoreType.DMA((n - 1,)),
            pltpu.SemaphoreType.DMA((n - 1,)),
        ],
        compiler_params=pltpu.CompilerParams(
            collective_id=0, has_side_effects=True, vmem_limit_bytes=24 << 20
        ),
        cost_estimate=pl.CostEstimate(
            flops=200 * channels * length, bytes_accessed=12 * channels * length, transcendentals=0
        ),
        name="mixer",
    )(x, halo, bg, extra, taps, rate, wr, wa)


def layer_kernel(
    n, split,
    x_ref, bg_ref, extra_ref, taps_ref, dp_ref, wr_ref, wa_ref, ow_ref, res_ref, gain_ref,
    gw_ref, uw_ref, dw_ref,
    out_ref,
    x_s, bg_s, extra_s, ow_s, res_s, raw_s, pack_s,
    xt_s, halo_s, wbd_s, a_s, b_s, ea_s, eb_s, act_s, ends_s, all_s, in_s, mix_s,
    part_s, part_r, mid_s, tok_s, wide_s, hid_s, ff_s, tp_s, red_s, rz_s,
    in_sem, hs_sem, hr_sem, ss_sem, sr_sem,
    zs_sem, zr_sem, ps_sem, pr_sem, fs_sem, fr_sem, rs_sem, rr_sem,
    bs_sem, br_sem, ts_sem, tr_sem, cs_sem, cr_sem,
    as_sem, ar_sem, ks_sem, kr_sem, os_sem, or_sem,
):
    me = lax.axis_index("sp")
    core = lax.axis_index("tp")
    plane = n // split
    rank, spot = me // plane, lax.rem(me, plane)
    f32, bf16 = jnp.float32, jnp.bfloat16
    channels, length = x_s.shape
    groups = channels // LANES
    block = wr_ref.shape[1]
    taps = taps_ref.shape[0]
    kinds, full, depth = pack_s.shape
    span = full // split
    width = mid_s.shape[1]
    barrier = pltpu.get_barrier_semaphore()

    raw_refs = (gw_ref, uw_ref, dw_ref)
    loads = [
        pltpu.make_async_copy(src, dst, in_sem.at[i])
        for i, (src, dst) in enumerate(
            [
                (x_ref, x_s),
                (gw_ref, raw_s.at[0]),
                (uw_ref, raw_s.at[1]),
                (dw_ref, raw_s.at[2]),
                (extra_ref, extra_s),
                (bg_ref, bg_s),
                (ow_ref, ow_s),
                (res_ref, res_s),
            ]
        )
    ]
    for load in loads:
        load.start()

    def greet(k, carry):
        pl.semaphore_signal(
            barrier, inc=1, device_id={"sp": lax.rem(me + k, n)}, device_id_type=MESH
        )
        return carry

    lax.fori_loop(1, n, greet, 0)
    pl.semaphore_signal(barrier, inc=1, device_id={"tp": 1 - core}, device_id_type=MESH)

    def remote(src, dst, ssem, rsem, where):
        return pltpu.make_async_remote_copy(
            src_ref=src, dst_ref=dst, send_sem=ssem, recv_sem=rsem,
            device_id=where, device_id_type=MESH,
        )

    def lanes(i):
        return pl.ds(pl.multiple_of(i * LANES, LANES), LANES)

    def own(c):
        return pack_s.at[c, pl.ds(pl.multiple_of(rank * span, span), span)]

    def window(c, source):
        return wide_s.at[c, :, lanes(source)]

    side = rank // 2
    inner = lax.rem(rank, 2) + side - 2 * lax.rem(rank, 2) * side
    mate = rank + 1 - 2 * lax.rem(rank, 2)
    ahead = rank + 1 - 2 * side

    def away(k):
        if k < 2:
            return (rank, mate)[k]
        t = 2 if k == 2 else 3
        return t + side * (split - 1 - 2 * t)

    def there(k):
        return k if k < 2 else 3 - inner

    def z_copy(c, k):
        to = away(k)
        return remote(
            pack_s.at[c, pl.ds(pl.multiple_of(to * span, span), span)], window(c, me),
            zs_sem.at[c, k - 1], zr_sem.at[c, there(k) - 1], {"sp": to * plane + spot},
        )

    def z_landed(c, k):
        source = away(k) * plane + spot
        return remote(
            own(c), window(c, source), zs_sem.at[c, k - 1], zr_sem.at[c, k - 1], {"sp": source}
        )

    def beside(m):
        return spot + 1 - 2 * lax.rem(spot, 2) if m == 1 else spot + 2 - 4 * (spot // 2)

    def pass_copy(c, k, m):
        source = away(k) * plane + spot
        return remote(
            window(c, source) if k else own(c), window(c, source),
            fs_sem.at[c, k, m - 1], fr_sem.at[c, k, m - 1], {"sp": rank * plane + beside(m)},
        )

    def pass_landed(c, k, m):
        source = away(k) * plane + beside(m)
        return remote(
            window(c, source), window(c, source),
            fs_sem.at[c, k, m - 1], fr_sem.at[c, k, m - 1], {"sp": rank * plane + beside(m)},
        )

    def relay_window(c, k, m, where):
        source = away(k) * plane + where
        return wide_s.at[c, pl.ds((m - 1) * (span // 2), span // 2), lanes(source)]

    def relay_copy(c, k, m):
        view = relay_window(c, k, m, beside(m))
        return remote(
            view, view, rs_sem.at[c, k, m - 1], rr_sem.at[c, k, m - 1],
            {"sp": rank * plane + beside(3 - m)},
        )

    def relay_landed(c, k, m):
        view = relay_window(c, k, m, 3 - spot)
        return remote(
            view, view, rs_sem.at[c, k, m - 1], rr_sem.at[c, k, m - 1],
            {"sp": rank * plane + beside(3 - m)},
        )

    def z_start(c):
        @pl.when(inner == 0)
        def _():
            z_copy(c, 1).start()

        for k in range(2, split):
            z_copy(c, k).start()

    def z_mate(c):
        @pl.when(inner == 1)
        def _():
            z_copy(c, 1).start()

    def spread(c, k):
        if k:
            z_landed(c, k).wait_recv()
        for m in (1, 2):
            pass_copy(c, k, m).start()

    def relay(c, k):
        for m in (1, 2):
            pass_landed(c, k, m).wait_recv()
            relay_copy(c, k, m).start()

    def settle(c, k):
        for m in (1, 2):
            relay_landed(c, k, m).wait_recv()

    def turn(c):
        loads[1 + c].wait()

        def step(j, carry):
            pack_s[c, lanes(j), :] = raw_s[c, :, lanes(j)].T
            return carry

        lax.fori_loop(0, full // LANES, step, 0)

    def keep(c):
        wide_s[c, :, lanes(me)] = own(c)[...]

    loads[0].wait()

    def flip(g, carry):
        xt_s[pl.ds(8, length), lanes(g)] = x_s[lanes(g), :].astype(f32).T
        return carry

    lax.fori_loop(0, groups, flip, 0)
    turn(0)
    pl.semaphore_wait(barrier, n)
    halo = remote(
        xt_s.at[pl.ds(length, 8), :], halo_s, hs_sem, hr_sem, {"sp": lax.rem(me + 1, n)}
    )
    halo.start()
    z_mate(0)
    z_start(0)
    spread(0, 0)
    turn(1)
    spread(1, 0)
    turn(2)
    for c in range(kinds):
        keep(c)

    rowb = lax.broadcasted_iota(jnp.int32, (LANES, LANES), 0) // block
    colb = lax.broadcasted_iota(jnp.int32, (LANES, LANES), 1) // block
    eye_r = lax.broadcasted_iota(jnp.int32, (block, LANES), 0)
    eye_c = lax.rem(lax.broadcasted_iota(jnp.int32, (block, LANES), 1), block)
    twice = jnp.where(eye_r == eye_c, 1.0, 0.0).astype(bf16)

    def widen(g, carry):
        for slot, w_ref in ((0, wr_ref), (1, wa_ref)):
            pair = jnp.concatenate([w_ref[2 * g], w_ref[2 * g + 1]], axis=0)
            both = jnp.dot(pair, twice, preferred_element_type=f32)
            wbd_s[g, :, slot * LANES : (slot + 1) * LANES] = jnp.where(
                rowb == colb, both, 0.0
            ).astype(bf16)
        return carry

    lax.fori_loop(0, groups, widen, 0)
    loads[4].wait()
    halo.wait()
    xt_s[0:8, :] = halo_s[...] * jnp.where(me > 0, 1.0, 0.0)

    octets = length // 8
    sub = lax.broadcasted_iota(jnp.int32, (octets, 8, LANES), 1)
    row = lax.broadcasted_iota(jnp.int32, (octets, LANES), 0)

    def local(g, carry):
        cols = lanes(g)
        tap = taps_ref[:, cols].astype(f32)
        total = tap[taps - 1 : taps] * xt_s[pl.ds(8, length), cols]
        for k in range(taps - 2, -1, -1):
            total = total + tap[k : k + 1] * xt_s[pl.ds(9 - taps + k, length), cols]
        conv = total.astype(bf16)
        both = jnp.dot(conv, wbd_s[g], preferred_element_type=f32)
        recur = jax.nn.sigmoid(both[:, :LANES])
        admit = jax.nn.sigmoid(both[:, LANES:])
        rate = -8.0 * jax.nn.softplus(-dp_ref[pl.ds(g, 1), :])
        log_decay = recur * rate + extra_s[lanes(g), :].T
        a = jnp.exp(log_decay)
        b = jnp.sqrt(neg_expm1(2.0 * log_decay)) * admit * conv.astype(f32)
        a = a.reshape(octets, 8, LANES)
        b = b.reshape(octets, 8, LANES)
        for shift in (1, 2, 4):
            seen = sub >= shift
            b = b + a * jnp.where(seen, pltpu.roll(b, shift, 1), 0.0)
            a = a * jnp.where(seen, pltpu.roll(a, shift, 1), 1.0)
        a_s[g] = a.reshape(length, LANES)
        b_s[g] = b.reshape(length, LANES)
        ea = a_s[g, pl.ds(7, octets, stride=8), :]
        eb = b_s[g, pl.ds(7, octets, stride=8), :]
        shift = 1
        while shift < octets:
            seen = row >= shift
            eb = eb + ea * jnp.where(seen, pltpu.roll(eb, shift, 0), 0.0)
            ea = ea * jnp.where(seen, pltpu.roll(ea, shift, 0), 1.0)
            shift *= 2
        ends_s[pl.ds(g, 1), :] = ea[octets - 1 :]
        ends_s[pl.ds(groups + g, 1), :] = eb[octets - 1 :]
        ea_s[g] = jnp.where(row >= 1, pltpu.roll(ea, 1, 0), 1.0)
        eb_s[g] = jnp.where(row >= 1, pltpu.roll(eb, 1, 0), 0.0)
        return carry

    lax.fori_loop(0, groups, local, 0)

    def state(k):
        return remote(
            ends_s, all_s.at[k - 1], ss_sem.at[k - 1], sr_sem.at[k - 1],
            {"sp": lax.rem(me + k, n)},
        )

    def state_send(k, carry):
        state(k).start()
        return carry

    lax.fori_loop(1, n - me, state_send, 0)
    z_start(1)
    z_start(2)
    spread(0, 1)
    relay(0, 0)
    spread(2, 0)
    loads[5].wait()

    def gelu(g, carry):
        v = bg_s[lanes(g), :].astype(f32).T
        act_s[g] = 0.5 * v * (1.0 + jnp.tanh(0.7978845608028654 * (v + 0.044715 * v * v * v)))
        return carry

    lax.fori_loop(0, groups, gelu, 0)
    relay(1, 0)
    z_mate(1)
    spread(0, 2)
    relay(0, 1)
    spread(0, 3)
    relay(2, 0)
    z_mate(2)
    spread(1, 1)

    def state_wait(k, carry):
        remote(
            ends_s, all_s.at[k - 1], ss_sem.at[k - 1], sr_sem.at[k - 1],
            {"sp": lax.rem(me - k + n, n)},
        ).wait_recv()
        return carry

    lax.fori_loop(1, me + 1, state_wait, 0)

    def state_sent(k, carry):
        state(k).wait_send()
        return carry

    def fold(i, before):
        part = all_s[me - 1 - i]
        return part[:groups] * before + part[groups:]

    in_s[...] = lax.fori_loop(0, me, fold, jnp.zeros((groups, LANES), f32))

    def close(g, carry):
        enter = eb_s[g] + ea_s[g] * in_s[pl.ds(g, 1), :]
        states = jnp.concatenate(
            [
                b_s[g, i * 8 : i * 8 + 8, :] + a_s[g, i * 8 : i * 8 + 8, :] * enter[i : i + 1]
                for i in range(octets)
            ],
            axis=0,
        )
        mix_s[:, lanes(g)] = (states * act_s[g]).astype(bf16)
        return carry

    lax.fori_loop(0, groups, close, 0)

    pieces, row_count, cut = part_s.shape

    def swap(i):
        return remote(
            part_s.at[i], part_r.at[i], bs_sem.at[i], br_sem.at[i], {"tp": 1 - core}
        )

    loads[6].wait()
    for i in range(pieces):
        part_s[i] = jnp.dot(
            mix_s[...], ow_s[:, i * cut : (i + 1) * cut], preferred_element_type=f32
        ).astype(bf16)
        swap(i).start()
    relay(0, 2)
    loads[7].wait()
    square = jnp.zeros((row_count, 1), f32)
    for i in range(pieces):
        swap(i).wait()
        cols = slice(i * cut, (i + 1) * cut)
        branch = part_s[i].astype(f32) + part_r[i].astype(f32)
        middle = (res_s[:, cols].astype(f32) + branch).astype(bf16)
        mid_s[:, cols] = middle
        middle = middle.astype(f32)
        square = square + jnp.sum(middle * middle, axis=1, keepdims=True)
    scale = lax.rsqrt(square * (1.0 / (pieces * cut)) + 1e-06)
    for i in range(width // LANES):
        cols = slice(i * LANES, (i + 1) * LANES)
        gain = gain_ref[i : i + 1, :].astype(f32)
        tok_s[rank, :, cols] = (mid_s[:, cols].astype(f32) * scale * gain).astype(bf16)

    half = row_count // 2
    mine = pl.ds(pl.multiple_of(core * half, half), half)
    other = pl.ds(pl.multiple_of((1 - core) * half, half), half)

    bits = ts_sem.shape[2]
    bit = half // bits

    def some(which, p):
        return pl.ds(pl.multiple_of(which * half + p * bit, bit), bit)

    def tok_copy(way, d, p):
        step = 1 - 2 * way
        view = tok_s.at[rank - (d - 1) * step, some(core, p), :]
        return remote(
            view, view, ts_sem.at[way, d - 1, p], tr_sem.at[way, d - 1, p],
            {"sp": (rank + step) * plane + spot},
        )

    def tok_landed(way, d, p):
        step = 1 - 2 * way
        view = tok_s.at[rank - d * step, some(core, p), :]
        return remote(
            view, view, ts_sem.at[way, d - 1, p], tr_sem.at[way, d - 1, p],
            {"sp": (rank - step) * plane + spot},
        )

    def tok_pass(way, d, p, which):
        view = tok_s.at[rank - d * (1 - 2 * way), some(which, p), :]
        return remote(
            view, view, cs_sem.at[way, d - 1, p], cr_sem.at[way, d - 1, p], {"tp": 1 - core}
        )

    def held(way, d):
        return rank >= d if way == 0 else rank <= split - 1 - d

    def onward(way, d):
        return (
            jnp.logical_and(rank >= d, rank < split - 1)
            if way == 0
            else jnp.logical_and(rank <= split - 1 - d, rank > 0)
        )

    def tok_start():
        for way in (0, 1):

            @pl.when(onward(way, 0))
            def _():
                for p in range(bits):
                    tok_copy(way, 1, p).start()

    def tok_relay(d, close, p):
        for way in (0, 1):
            here = lax.rem(rank, 2) == (1 - way if close else way)

            @pl.when(jnp.logical_and(held(way, d), here))
            def _():
                tok_landed(way, d, p).wait_recv()
                tok_pass(way, d, p, core).start()

            if d < split - 1:

                @pl.when(jnp.logical_and(onward(way, d), here))
                def _():
                    tok_copy(way, d + 1, p).start()

    def tok_ready(d, close):
        for way in (0, 1):
            here = lax.rem(rank, 2) == (1 - way if close else way)

            @pl.when(jnp.logical_and(held(way, d), here))
            def _():
                for p in range(bits):
                    tok_pass(way, d, p, 1 - core).wait_recv()

    chunks, _, chunk = ff_s.shape[1:]
    across = (((1,), (1,)), ((), ()))

    def target(i):
        t = (1 + inner, 2 - 2 * inner, 3, inner)[i]
        return t + side * (split - 1 - 2 * t)

    per = chunks // split

    def col(j, back=False):
        t = split - 1 - j // per if back else j // per
        return (t + side * (split - 1 - 2 * t)) * per + j % per

    def near(j):
        return away(j // per) * per + j % per

    def hid(i):
        tokens = tok_s[target(i)]
        gate = lax.dot_general(tokens, wide_s[0], across, preferred_element_type=f32)
        up = lax.dot_general(tokens, wide_s[1], across, preferred_element_type=f32)
        hid_s[i] = (gate / (1.0 + jnp.exp(-gate)) * up).astype(bf16)

    def offer(i, js):
        js = list(js)
        for at in range(len(js) + 1):
            if at < len(js):
                part(i, near(js[at]))
            if at:
                lead(i, near(js[at - 1]))

    def tp_copy(i, q):
        return remote(
            ff_s.at[i, q, other, :], tp_s.at[i, q], as_sem.at[i, q], ar_sem.at[i, q],
            {"tp": 1 - core},
        )

    def part(i, q):
        cols = pl.ds(pl.multiple_of(q * chunk, chunk), chunk)
        ff_s[i, q] = jnp.dot(
            hid_s[i], wide_s[2, :, cols], preferred_element_type=f32
        ).astype(bf16)
        tp_copy(i, q).start()

    def sum_copy(a, slot, q, to):
        return remote(
            red_s.at[a, q], rz_s.at[slot, q], ks_sem.at[a, q], kr_sem.at[slot, q],
            {"sp": to * plane + spot},
        )

    def pair(i, q):
        tp_copy(i, q).wait()
        return ff_s[i, q, mine, :].astype(f32) + tp_s[i, q].astype(f32)

    def summed(i, slots, q):
        mixed = pair(i, q)
        for slot in slots:
            sum_copy(0, slot, q, mate).wait_recv()
            mixed = mixed + rz_s[slot, q].astype(f32)
        return mixed

    def lead(i, q):
        red_s[i, q] = summed(i, (), q).astype(bf16)
        sum_copy(i, i, q, mate).start()

    follow = ((0, 1, 3), (2, 2, 4), (1, 4, 3))

    def trail(a, q):
        i, slot, out_slot = follow[a]
        red_s[a, q] = summed(i, (slot,), q).astype(bf16)
        sum_copy(a, out_slot, q, ahead if a < 2 else mate).start()

    def out_copy(q):
        view = out_ref.at[mine, pl.ds(pl.multiple_of(q * chunk, chunk), chunk)]
        return remote(view, view, os_sem.at[q], or_sem.at[q], {"tp": 1 - core})

    def out_landed(q):
        view = out_ref.at[other, pl.ds(pl.multiple_of(q * chunk, chunk), chunk)]
        return remote(view, view, os_sem.at[q], or_sem.at[q], {"tp": 1 - core})

    def finish(role, q):
        cols = pl.ds(pl.multiple_of(q * chunk, chunk), chunk)
        total = summed(split - 1, (0, 3) if role else (3,), q)
        out_ref[mine, cols] = (mid_s[mine, cols].astype(f32) + total).astype(bf16)
        out_copy(q).start()

    first = range(2 * per)
    second = range(2 * per, chunks)

    tok_start()
    relay(0, 3)
    spread(1, 2)
    relay(1, 1)
    spread(1, 3)
    relay(1, 2)
    spread(2, 1)
    relay(1, 3)
    spread(2, 2)

    @pl.when(inner == 0)
    def outer_plane():
        for p in range(bits):
            tok_relay(1, True, p)
        for c in (0, 1):
            for k in range(split):
                settle(c, k)
        tok_ready(1, True)
        hid(0)
        relay(2, 1)
        settle(2, 0)
        offer(0, range(per))
        spread(2, 3)
        relay(2, 2)
        settle(2, 1)
        offer(0, range(per, 2 * per))
        relay(2, 3)
        for p in range(bits):
            tok_relay(2, True, p)
        tok_ready(2, True)
        hid(1)
        offer(1, first)
        settle(2, 2)
        offer(1, range(2 * per, 3 * per))
        settle(2, 3)
        offer(1, range(3 * per, chunks))
        for j in second:
            part(0, near(j))
        for p in range(bits):
            tok_relay(3, True, p)
        tok_ready(3, True)
        hid(2)
        offer(2, range(chunks))
        for j in second:
            lead(0, near(j))
        hid(3)
        for j in range(chunks):
            part(3, near(j))
        for j in range(chunks):
            finish(0, col(j, True))

    @pl.when(inner == 1)
    def inner_plane():
        relay(2, 1)
        for p in range(bits):
            tok_relay(1, True, p)
        for c in (0, 1):
            for k in range(split):
                settle(c, k)
        for p in range(bits):
            tok_relay(1, False, p)
        spread(2, 3)
        relay(2, 2)
        tok_ready(1, True)
        tok_ready(1, False)
        hid(0)
        relay(2, 3)
        hid(3)
        for p in range(bits):
            tok_relay(2, False, p)
        hid(1)
        for k in range(split):
            settle(2, k)
        for j in range(chunks):
            part(0, col(j))
        tok_ready(2, False)
        for j in range(chunks):
            part(1, col(j))
        hid(2)
        for j in range(chunks):
            trail(0, col(j))
        for j in range(chunks):
            part(2, col(j))
        for j in range(chunks):
            part(3, col(j))
        lag = chunks // 2
        for j in range(chunks + lag):
            if j < chunks:
                trail(1, col(j))
            if j >= lag:
                trail(2, col(j - lag, True))
        for j in range(chunks):
            finish(1, col(j))

    lax.fori_loop(1, n - me, state_sent, 0)
    for q in range(chunks):
        out_copy(q).wait_send()
        out_landed(q).wait_recv()
        for a in range(split - 1):
            sum_copy(a, a, q, mate).wait_send()
    for way in (0, 1):
        for d in range(1, split):

            @pl.when(onward(way, d - 1))
            def _():
                for p in range(bits):
                    tok_copy(way, d, p).wait_send()

            @pl.when(held(way, d))
            def _():
                for p in range(bits):
                    tok_pass(way, d, p, core).wait_send()

    for c in range(kinds):
        for k in range(split):
            for m in (1, 2):
                pass_copy(c, k, m).wait_send()
                relay_copy(c, k, m).wait_send()
            if k:
                z_copy(c, k).wait_send()


def layer(n, split, x, bg, extra, taps, dp, wr, wa, ow, res, gain, gw, uw, dw):
    channels, length = x.shape
    groups = channels // LANES
    rows, width = res.shape
    depth, full = gw.shape
    span = full // split
    kinds = 3
    cut = 512
    pieces = width // cut
    chunk = width // 4
    chunks = width // chunk
    half = rows // 2
    vmem = pl.BlockSpec(memory_space=pltpu.VMEM)
    hbm = pl.BlockSpec(memory_space=pl.ANY)
    dma = pltpu.SemaphoreType.DMA
    bf16, f32 = jnp.bfloat16, jnp.float32
    buf = pltpu.VMEM
    return pl.pallas_call(
        functools.partial(layer_kernel, n, split),
        out_shape=jax.ShapeDtypeStruct((rows, width), bf16),
        in_specs=[hbm, hbm, hbm, vmem, vmem, vmem, vmem, hbm, hbm, vmem, hbm, hbm, hbm],
        out_specs=vmem,
        scratch_shapes=[
            buf((channels, length), bf16),
            buf((channels, length), bf16),
            buf((channels, length), f32),
            buf((channels, width), bf16),
            buf((rows, width), bf16),
            buf((kinds, depth, full), bf16),
            buf((kinds, full, depth), bf16),
            buf((length + 8, channels), f32),
            buf((8, channels), f32),
            buf((groups, LANES, 2 * LANES), bf16),
            buf((groups, length, LANES), f32),
            buf((groups, length, LANES), f32),
            buf((groups, length // 8, LANES), f32),
            buf((groups, length // 8, LANES), f32),
            buf((groups, length, LANES), f32),
            buf((2 * groups, LANES), f32),
            buf((n - 1, 2 * groups, LANES), f32),
            buf((groups, LANES), f32),
            buf((length, channels), bf16),
            buf((pieces, rows, cut), bf16),
            buf((pieces, rows, cut), bf16),
            buf((rows, width), bf16),
            buf((split, rows, width), bf16),
            buf((kinds, span, width), bf16),
            buf((split, rows, span), bf16),
            buf((split, chunks, rows, chunk), bf16),
            buf((split, chunks, half, chunk), bf16),
            buf((split - 1, chunks, half, chunk), bf16),
            buf((5, chunks, half, chunk), bf16),
            dma((8,)),
            dma,
            dma,
            dma((n - 1,)),
            dma((n - 1,)),
            dma((kinds, split - 1)),
            dma((kinds, split - 1)),
            dma((1,)),
            dma((1,)),
            dma((kinds, split, 2)),
            dma((kinds, split, 2)),
            dma((kinds, split, 2)),
            dma((kinds, split, 2)),
            dma((pieces,)),
            dma((pieces,)),
            dma((2, split - 1, 2)),
            dma((2, split - 1, 2)),
            dma((2, split - 1, 2)),
            dma((2, split - 1, 2)),
            dma((split, chunks)),
            dma((split, chunks)),
            dma((split - 1, chunks)),
            dma((5, chunks)),
            dma((chunks,)),
            dma((chunks,)),
        ],
        compiler_params=pltpu.CompilerParams(
            collective_id=1, has_side_effects=True, vmem_limit_bytes=54 << 20
        ),
        name="layer",
    )(x, bg, extra, taps, dp, wr, wa, ow, res, gain, gw, uw, dw)


def on_device(
    residual_in,
    mixer_input,
    branch_gate,
    conv_taps,
    recur_weight,
    admit_weight,
    decay_param,
    decay_extra,
    out_weight,
    norm_gain,
    gate_weight,
    up_weight,
    down_weight,
):
    n = lax.axis_size("sp")
    length = mixer_input.shape[1]
    width, share_ff = residual_in.shape[1], gate_weight.shape[1]
    split = 4
    depth = gate_weight.shape[0]
    if (
        lax.axis_size("tp") == 2
        and n == 4 * split
        and depth == LANES
        and width == n * depth
        and share_ff % LANES == 0
        and share_ff % (32 * split) == 0
        and 2 * recur_weight.shape[1] == LANES
        and conv_taps.shape[1] <= 9
        and residual_in.shape[0] == length
        and length % (2 * LANES) == 0
    ):
        return layer(
            n,
            split,
            mixer_input,
            branch_gate,
            decay_extra,
            conv_taps.T,
            decay_param.reshape(-1, LANES),
            recur_weight,
            admit_weight,
            out_weight,
            residual_in,
            norm_gain.reshape(-1, LANES),
            gate_weight,
            up_weight,
            down_weight,
        )
    halo = lax.ppermute(
        mixer_input[:, length - LANES :], "sp", [(i, i + 1) for i in range(n - 1)]
    )
    rate = -8.0 * jax.nn.softplus(-decay_param)[:, None]
    mixed_out = mixer(
        n,
        mixer_input,
        halo,
        branch_gate,
        decay_extra,
        conv_taps.astype(jnp.float32),
        rate,
        recur_weight.transpose(0, 2, 1),
        admit_weight.transpose(0, 2, 1),
    )
    row_count = residual_in.shape[0]
    partial_value = lax.dot_general(
        mixed_out, out_weight, (((0,), (0,)), ((), ())), preferred_element_type=jnp.float32
    )
    branch = lax.psum(partial_value.astype(jnp.bfloat16), "tp").astype(jnp.float32)
    middle = (residual_in.astype(jnp.float32) + branch).astype(jnp.bfloat16)
    middle_wide = middle.astype(jnp.float32)
    row_scale = lax.rsqrt(jnp.mean(middle_wide * middle_wide, axis=1, keepdims=True) + 1e-06)
    normed = (middle_wide * row_scale * norm_gain.astype(jnp.float32)).astype(jnp.bfloat16)
    gate_pre = jnp.dot(
        normed,
        lax.all_gather(gate_weight, "sp", axis=0, tiled=True),
        preferred_element_type=jnp.float32,
    )
    up_pre = jnp.dot(
        normed,
        lax.all_gather(up_weight, "sp", axis=0, tiled=True),
        preferred_element_type=jnp.float32,
    )
    down_whole = lax.all_gather(down_weight, "sp", axis=0, tiled=True)
    hidden = (jax.nn.silu(gate_pre) * up_pre).astype(jnp.bfloat16)
    share = row_count // lax.axis_size("tp")
    channel_out = lax.psum_scatter(
        lax.dot_general(
            hidden, down_whole, (((1,), (1,)), ((), ())), preferred_element_type=jnp.float32
        ).astype(jnp.bfloat16),
        "tp",
        scatter_dimension=0,
        tiled=True,
    ).astype(jnp.float32)
    first_row = lax.axis_index("tp") * share
    own_rows = lax.dynamic_slice_in_dim(middle, first_row, share, 0)
    layer_rows = (own_rows.astype(jnp.float32) + channel_out).astype(jnp.bfloat16)
    return lax.all_gather(layer_rows, "tp", axis=0, tiled=True)


def solution(mesh):
    placed = (
        P("sp", None),
        P("tp", "sp"),
        P("tp", "sp"),
        P("tp", None),
        P("tp", None, None),
        P("tp", None, None),
        P("tp"),
        P("tp", "sp"),
        P("tp", None),
        P(),
        P("sp", "tp"),
        P("sp", "tp"),
        P("sp", "tp"),
    )
    return jax.shard_map(
        on_device, mesh=mesh, in_specs=placed, out_specs=P("sp", None), check_vma=False
    )
```

```python
import functools

import jax
import jax.numpy as jnp
from jax import lax
from jax.experimental import pallas as pl
from jax.experimental.pallas import tpu as pltpu
from jax.sharding import PartitionSpec as P

MESH = pl.DeviceIdType.MESH
LANES = 128


def neg_expm1(v):
    series = jnp.full_like(v, 1.0)
    for k in range(9, 1, -1):
        series = 1.0 + series * v * (1.0 / k)
    return jnp.where(v > -0.5, -v * series, 1.0 - jnp.exp(v))


def mixer_kernel(
    n,
    x_ref,
    halo_ref,
    bg_ref,
    extra_ref,
    taps_ref,
    rate_ref,
    wr_ref,
    wa_ref,
    out_ref,
    state_s,
    run_s,
    ends_s,
    all_s,
    in_s,
    send_sem,
    recv_sem,
):
    me = lax.axis_index("sp")
    barrier = pltpu.get_barrier_semaphore()

    def greet(k, carry):
        pl.semaphore_signal(
            barrier, inc=1, device_id={"sp": lax.rem(me + k, n)}, device_id_type=MESH
        )
        return carry

    lax.fori_loop(1, n, greet, 0)
    channels, length = x_ref.shape
    block = wr_ref.shape[1]
    groups = channels // LANES
    tap_count = taps_ref.shape[1]
    lane = lax.broadcasted_iota(jnp.int32, (LANES, length), 1)

    def local(g, carry):
        rows = pl.ds(pl.multiple_of(g * LANES, LANES), LANES)
        wide = jnp.concatenate(
            [halo_ref[rows, :].astype(jnp.float32), x_ref[rows, :].astype(jnp.float32)], axis=1
        )
        taps = taps_ref[rows, :]
        total = taps[:, tap_count - 1 :] * wide[:, LANES:]
        for tap in range(tap_count - 2, -1, -1):
            total = total + taps[:, tap : tap + 1] * pltpu.roll(wide, tap_count - 1 - tap, 1)[:, LANES:]
        conv = total.astype(jnp.bfloat16)
        per = LANES // block
        recur, admit = [], []
        for b in range(per):
            part = conv[b * block : (b + 1) * block]
            recur.append(jnp.dot(wr_ref[g * per + b], part, preferred_element_type=jnp.float32))
            admit.append(jnp.dot(wa_ref[g * per + b], part, preferred_element_type=jnp.float32))
        recur = jax.nn.sigmoid(jnp.concatenate(recur, axis=0))
        admit = jax.nn.sigmoid(jnp.concatenate(admit, axis=0))
        log_decay = recur * rate_ref[rows, :] + extra_ref[rows, :]
        a = jnp.exp(log_decay)
        b = jnp.sqrt(neg_expm1(2.0 * log_decay)) * admit * conv.astype(jnp.float32)
        shift = 1
        while shift < length:
            seen = lane >= shift
            b = b + a * jnp.where(seen, pltpu.roll(b, shift, 1), 0.0)
            a = a * jnp.where(seen, pltpu.roll(a, shift, 1), 1.0)
            shift *= 2
        state_s[rows, :] = b
        run_s[rows, :] = a
        ends_s[pl.ds(g, 1), :] = a[:, length - LANES :].T[LANES - 1 :]
        ends_s[pl.ds(groups + g, 1), :] = b[:, length - LANES :].T[LANES - 1 :]
        return carry

    lax.fori_loop(0, groups, local, 0)
    pl.semaphore_wait(barrier, n - 1)

    def copy_to(k):
        return pltpu.make_async_remote_copy(
            src_ref=ends_s,
            dst_ref=all_s.at[k - 1],
            send_sem=send_sem.at[k - 1],
            recv_sem=recv_sem.at[k - 1],
            device_id={"sp": lax.rem(me + k, n)},
            device_id_type=MESH,
        )

    def send(k, carry):
        copy_to(k).start()
        return carry

    lax.fori_loop(1, n, send, 0)

    def finish(k, carry):
        copy_to(k).wait()
        return carry

    lax.fori_loop(1, n, finish, 0)

    def fold(i, before):
        k = n - 1 - i
        part = all_s[k - 1]
        new = part[:groups] * before + part[groups:]
        return jnp.where(k <= me, new, before)

    in_s[...] = lax.fori_loop(0, n - 1, fold, jnp.zeros((groups, LANES), jnp.float32))

    def close(g, carry):
        rows = pl.ds(pl.multiple_of(g * LANES, LANES), LANES)
        entering = jnp.broadcast_to(in_s[pl.ds(g, 1), :], (LANES, LANES)).T
        entering = jnp.concatenate([entering] * (length // LANES), axis=1)
        states = state_s[rows, :] + run_s[rows, :] * entering
        v = bg_ref[rows, :].astype(jnp.float32)
        act = 0.5 * v * (1.0 + jnp.tanh(0.7978845608028654 * (v + 0.044715 * v * v * v)))
        out_ref[rows, :] = (states * act).astype(jnp.bfloat16)
        return carry

    lax.fori_loop(0, groups, close, 0)


def mixer(n, x, halo, bg, extra, taps, rate, wr, wa):
    channels, length = x.shape
    groups = channels // LANES
    vmem = pl.BlockSpec(memory_space=pltpu.VMEM)
    return pl.pallas_call(
        functools.partial(mixer_kernel, n),
        out_shape=jax.ShapeDtypeStruct((channels, length), jnp.bfloat16),
        in_specs=[vmem] * 8,
        out_specs=vmem,
        scratch_shapes=[
            pltpu.VMEM((channels, length), jnp.float32),
            pltpu.VMEM((channels, length), jnp.float32),
            pltpu.VMEM((2 * groups, LANES), jnp.float32),
            pltpu.VMEM((n - 1, 2 * groups, LANES), jnp.float32),
            pltpu.VMEM((groups, LANES), jnp.float32),
            pltpu.SemaphoreType.DMA((n - 1,)),
            pltpu.SemaphoreType.DMA((n - 1,)),
        ],
        compiler_params=pltpu.CompilerParams(
            collective_id=0, has_side_effects=True, vmem_limit_bytes=24 << 20
        ),
        cost_estimate=pl.CostEstimate(
            flops=200 * channels * length, bytes_accessed=12 * channels * length, transcendentals=0
        ),
        name="mixer",
    )(x, halo, bg, extra, taps, rate, wr, wa)


def layer_kernel(
    n, split,
    x_ref, bg_ref, extra_ref, taps_ref, dp_ref, wr_ref, wa_ref, ow_ref, res_ref, gain_ref,
    gw_ref, uw_ref, dw_ref,
    out_ref,
    x_s, bg_s, extra_s, ow_s, res_s, raw_s, pack_s,
    xt_s, halo_s, wbd_s, a_s, b_s, ea_s, eb_s, act_s, ends_s, all_s, in_s, mix_s,
    part_s, part_r, mid_s, tok_s, wide_s, hid_s, ff_s, tp_s, red_s, rz_s,
    in_sem, hs_sem, hr_sem, ss_sem, sr_sem,
    zs_sem, zr_sem, ps_sem, pr_sem, fs_sem, fr_sem, rs_sem, rr_sem,
    bs_sem, br_sem, ts_sem, tr_sem, cs_sem, cr_sem,
    as_sem, ar_sem, ks_sem, kr_sem, os_sem, or_sem,
):
    me = lax.axis_index("sp")
    core = lax.axis_index("tp")
    plane = n // split
    rank, spot = me // plane, lax.rem(me, plane)
    f32, bf16 = jnp.float32, jnp.bfloat16
    channels, length = x_s.shape
    groups = channels // LANES
    block = wr_ref.shape[1]
    taps = taps_ref.shape[0]
    kinds, full, depth = pack_s.shape
    span = full // split
    width = mid_s.shape[1]
    barrier = pltpu.get_barrier_semaphore()

    raw_refs = (gw_ref, uw_ref, dw_ref)
    loads = [
        pltpu.make_async_copy(src, dst, in_sem.at[i])
        for i, (src, dst) in enumerate(
            [
                (x_ref, x_s),
                (gw_ref, raw_s.at[0]),
                (uw_ref, raw_s.at[1]),
                (dw_ref, raw_s.at[2]),
                (extra_ref, extra_s),
                (bg_ref, bg_s),
                (ow_ref, ow_s),
                (res_ref, res_s),
            ]
        )
    ]
    for load in loads:
        load.start()

    def greet(k, carry):
        pl.semaphore_signal(
            barrier, inc=1, device_id={"sp": lax.rem(me + k, n)}, device_id_type=MESH
        )
        return carry

    lax.fori_loop(1, n, greet, 0)
    pl.semaphore_signal(barrier, inc=1, device_id={"tp": 1 - core}, device_id_type=MESH)

    def remote(src, dst, ssem, rsem, where):
        return pltpu.make_async_remote_copy(
            src_ref=src, dst_ref=dst, send_sem=ssem, recv_sem=rsem,
            device_id=where, device_id_type=MESH,
        )

    def lanes(i):
        return pl.ds(pl.multiple_of(i * LANES, LANES), LANES)

    def own(c):
        return pack_s.at[c, pl.ds(pl.multiple_of(rank * span, span), span)]

    def window(c, source):
        return wide_s.at[c, :, lanes(source)]

    side = rank // 2
    inner = lax.rem(rank, 2) + side - 2 * lax.rem(rank, 2) * side
    mate = rank + 1 - 2 * lax.rem(rank, 2)
    ahead = rank + 1 - 2 * side

    def away(k):
        if k < 2:
            return (rank, mate)[k]
        t = 2 if k == 2 else 3
        return t + side * (split - 1 - 2 * t)

    def there(k):
        return k if k < 2 else 3 - inner

    def z_copy(c, k):
        to = away(k)
        return remote(
            pack_s.at[c, pl.ds(pl.multiple_of(to * span, span), span)], window(c, me),
            zs_sem.at[c, k - 1], zr_sem.at[c, there(k) - 1], {"sp": to * plane + spot},
        )

    def z_landed(c, k):
        source = away(k) * plane + spot
        return remote(
            own(c), window(c, source), zs_sem.at[c, k - 1], zr_sem.at[c, k - 1], {"sp": source}
        )

    def beside(m):
        return spot + 1 - 2 * lax.rem(spot, 2) if m == 1 else spot + 2 - 4 * (spot // 2)

    def pass_copy(c, k, m):
        source = away(k) * plane + spot
        return remote(
            window(c, source) if k else own(c), window(c, source),
            fs_sem.at[c, k, m - 1], fr_sem.at[c, k, m - 1], {"sp": rank * plane + beside(m)},
        )

    def pass_landed(c, k, m):
        source = away(k) * plane + beside(m)
        return remote(
            window(c, source), window(c, source),
            fs_sem.at[c, k, m - 1], fr_sem.at[c, k, m - 1], {"sp": rank * plane + beside(m)},
        )

    def relay_window(c, k, m, where):
        source = away(k) * plane + where
        return wide_s.at[c, pl.ds((m - 1) * (span // 2), span // 2), lanes(source)]

    def relay_copy(c, k, m):
        view = relay_window(c, k, m, beside(m))
        return remote(
            view, view, rs_sem.at[c, k, m - 1], rr_sem.at[c, k, m - 1],
            {"sp": rank * plane + beside(3 - m)},
        )

    def relay_landed(c, k, m):
        view = relay_window(c, k, m, 3 - spot)
        return remote(
            view, view, rs_sem.at[c, k, m - 1], rr_sem.at[c, k, m - 1],
            {"sp": rank * plane + beside(3 - m)},
        )

    def z_start(c):
        @pl.when(inner == 0)
        def _():
            z_copy(c, 1).start()

        for k in range(2, split):
            z_copy(c, k).start()

    def z_mate(c):
        @pl.when(inner == 1)
        def _():
            z_copy(c, 1).start()

    def spread(c, k):
        if k:
            z_landed(c, k).wait_recv()
        for m in (1, 2):
            pass_copy(c, k, m).start()

    def relay(c, k):
        for m in (1, 2):
            pass_landed(c, k, m).wait_recv()
            relay_copy(c, k, m).start()

    def settle(c, k):
        for m in (1, 2):
            relay_landed(c, k, m).wait_recv()

    def turn(c):
        loads[1 + c].wait()

        def step(j, carry):
            pack_s[c, lanes(j), :] = raw_s[c, :, lanes(j)].T
            return carry

        lax.fori_loop(0, full // LANES, step, 0)

    def keep(c):
        wide_s[c, :, lanes(me)] = own(c)[...]

    loads[0].wait()

    def flip(g, carry):
        xt_s[pl.ds(8, length), lanes(g)] = x_s[lanes(g), :].astype(f32).T
        return carry

    lax.fori_loop(0, groups, flip, 0)
    turn(0)
    pl.semaphore_wait(barrier, n)
    halo = remote(
        xt_s.at[pl.ds(length, 8), :], halo_s, hs_sem, hr_sem, {"sp": lax.rem(me + 1, n)}
    )
    halo.start()
    z_mate(0)
    z_start(0)
    spread(0, 0)
    turn(1)
    spread(1, 0)
    turn(2)
    for c in range(kinds):
        keep(c)

    rowb = lax.broadcasted_iota(jnp.int32, (LANES, LANES), 0) // block
    colb = lax.broadcasted_iota(jnp.int32, (LANES, LANES), 1) // block
    eye_r = lax.broadcasted_iota(jnp.int32, (block, LANES), 0)
    eye_c = lax.rem(lax.broadcasted_iota(jnp.int32, (block, LANES), 1), block)
    twice = jnp.where(eye_r == eye_c, 1.0, 0.0).astype(bf16)

    def widen(g, carry):
        for slot, w_ref in ((0, wr_ref), (1, wa_ref)):
            pair = jnp.concatenate([w_ref[2 * g], w_ref[2 * g + 1]], axis=0)
            both = jnp.dot(pair, twice, preferred_element_type=f32)
            wbd_s[g, :, slot * LANES : (slot + 1) * LANES] = jnp.where(
                rowb == colb, both, 0.0
            ).astype(bf16)
        return carry

    lax.fori_loop(0, groups, widen, 0)
    loads[4].wait()
    halo.wait()
    xt_s[0:8, :] = halo_s[...] * jnp.where(me > 0, 1.0, 0.0)

    octets = length // 8
    sub = lax.broadcasted_iota(jnp.int32, (octets, 8, LANES), 1)
    row = lax.broadcasted_iota(jnp.int32, (octets, LANES), 0)

    def local(g, carry):
        cols = lanes(g)
        tap = taps_ref[:, cols].astype(f32)
        total = tap[taps - 1 : taps] * xt_s[pl.ds(8, length), cols]
        for k in range(taps - 2, -1, -1):
            total = total + tap[k : k + 1] * xt_s[pl.ds(9 - taps + k, length), cols]
        conv = total.astype(bf16)
        both = jnp.dot(conv, wbd_s[g], preferred_element_type=f32)
        recur = jax.nn.sigmoid(both[:, :LANES])
        admit = jax.nn.sigmoid(both[:, LANES:])
        rate = -8.0 * jax.nn.softplus(-dp_ref[pl.ds(g, 1), :])
        log_decay = recur * rate + extra_s[lanes(g), :].T
        a = jnp.exp(log_decay)
        b = jnp.sqrt(neg_expm1(2.0 * log_decay)) * admit * conv.astype(f32)
        a = a.reshape(octets, 8, LANES)
        b = b.reshape(octets, 8, LANES)
        for shift in (1, 2, 4):
            seen = sub >= shift
            b = b + a * jnp.where(seen, pltpu.roll(b, shift, 1), 0.0)
            a = a * jnp.where(seen, pltpu.roll(a, shift, 1), 1.0)
        a_s[g] = a.reshape(length, LANES)
        b_s[g] = b.reshape(length, LANES)
        ea = a_s[g, pl.ds(7, octets, stride=8), :]
        eb = b_s[g, pl.ds(7, octets, stride=8), :]
        shift = 1
        while shift < octets:
            seen = row >= shift
            eb = eb + ea * jnp.where(seen, pltpu.roll(eb, shift, 0), 0.0)
            ea = ea * jnp.where(seen, pltpu.roll(ea, shift, 0), 1.0)
            shift *= 2
        ends_s[pl.ds(g, 1), :] = ea[octets - 1 :]
        ends_s[pl.ds(groups + g, 1), :] = eb[octets - 1 :]
        ea_s[g] = jnp.where(row >= 1, pltpu.roll(ea, 1, 0), 1.0)
        eb_s[g] = jnp.where(row >= 1, pltpu.roll(eb, 1, 0), 0.0)
        return carry

    lax.fori_loop(0, groups, local, 0)

    def state(k):
        return remote(
            ends_s, all_s.at[k - 1], ss_sem.at[k - 1], sr_sem.at[k - 1],
            {"sp": lax.rem(me + k, n)},
        )

    def state_send(k, carry):
        state(k).start()
        return carry

    lax.fori_loop(1, n - me, state_send, 0)
    z_start(1)
    spread(0, 1)
    relay(0, 0)
    spread(2, 0)
    loads[5].wait()

    def gelu(g, carry):
        v = bg_s[lanes(g), :].astype(f32).T
        act_s[g] = 0.5 * v * (1.0 + jnp.tanh(0.7978845608028654 * (v + 0.044715 * v * v * v)))
        return carry

    lax.fori_loop(0, groups, gelu, 0)
    relay(1, 0)
    z_mate(1)
    spread(0, 2)
    relay(0, 1)
    spread(0, 3)
    relay(2, 0)
    z_mate(2)
    spread(1, 1)

    def state_wait(k, carry):
        remote(
            ends_s, all_s.at[k - 1], ss_sem.at[k - 1], sr_sem.at[k - 1],
            {"sp": lax.rem(me - k + n, n)},
        ).wait_recv()
        return carry

    lax.fori_loop(1, me + 1, state_wait, 0)

    def state_sent(k, carry):
        state(k).wait_send()
        return carry

    def fold(i, before):
        part = all_s[me - 1 - i]
        return part[:groups] * before + part[groups:]

    in_s[...] = lax.fori_loop(0, me, fold, jnp.zeros((groups, LANES), f32))

    def close(g, carry):
        enter = eb_s[g] + ea_s[g] * in_s[pl.ds(g, 1), :]
        states = jnp.concatenate(
            [
                b_s[g, i * 8 : i * 8 + 8, :] + a_s[g, i * 8 : i * 8 + 8, :] * enter[i : i + 1]
                for i in range(octets)
            ],
            axis=0,
        )
        mix_s[:, lanes(g)] = (states * act_s[g]).astype(bf16)
        return carry

    lax.fori_loop(0, groups, close, 0)

    pieces, row_count, cut = part_s.shape

    def swap(i):
        return remote(
            part_s.at[i], part_r.at[i], bs_sem.at[i], br_sem.at[i], {"tp": 1 - core}
        )

    loads[6].wait()
    for i in range(pieces):
        part_s[i] = jnp.dot(
            mix_s[...], ow_s[:, i * cut : (i + 1) * cut], preferred_element_type=f32
        ).astype(bf16)
        swap(i).start()
    z_start(2)
    relay(0, 2)
    loads[7].wait()
    square = jnp.zeros((row_count, 1), f32)
    for i in range(pieces):
        swap(i).wait()
        cols = slice(i * cut, (i + 1) * cut)
        branch = part_s[i].astype(f32) + part_r[i].astype(f32)
        middle = (res_s[:, cols].astype(f32) + branch).astype(bf16)
        mid_s[:, cols] = middle
        middle = middle.astype(f32)
        square = square + jnp.sum(middle * middle, axis=1, keepdims=True)
    scale = lax.rsqrt(square * (1.0 / (pieces * cut)) + 1e-06)
    for i in range(width // LANES):
        cols = slice(i * LANES, (i + 1) * LANES)
        gain = gain_ref[i : i + 1, :].astype(f32)
        tok_s[rank, :, cols] = (mid_s[:, cols].astype(f32) * scale * gain).astype(bf16)

    half = row_count // 2
    mine = pl.ds(pl.multiple_of(core * half, half), half)
    other = pl.ds(pl.multiple_of((1 - core) * half, half), half)

    bits = ts_sem.shape[2]
    bit = half // bits

    def some(which, p):
        return pl.ds(pl.multiple_of(which * half + p * bit, bit), bit)

    def tok_copy(way, d, p):
        step = 1 - 2 * way
        view = tok_s.at[rank - (d - 1) * step, some(core, p), :]
        return remote(
            view, view, ts_sem.at[way, d - 1, p], tr_sem.at[way, d - 1, p],
            {"sp": (rank + step) * plane + spot},
        )

    def tok_landed(way, d, p):
        step = 1 - 2 * way
        view = tok_s.at[rank - d * step, some(core, p), :]
        return remote(
            view, view, ts_sem.at[way, d - 1, p], tr_sem.at[way, d - 1, p],
            {"sp": (rank - step) * plane + spot},
        )

    def tok_pass(way, d, p, which):
        view = tok_s.at[rank - d * (1 - 2 * way), some(which, p), :]
        return remote(
            view, view, cs_sem.at[way, d - 1, p], cr_sem.at[way, d - 1, p], {"tp": 1 - core}
        )

    def held(way, d):
        return rank >= d if way == 0 else rank <= split - 1 - d

    def onward(way, d):
        return (
            jnp.logical_and(rank >= d, rank < split - 1)
            if way == 0
            else jnp.logical_and(rank <= split - 1 - d, rank > 0)
        )

    def tok_start():
        for way in (0, 1):

            @pl.when(onward(way, 0))
            def _():
                for p in range(bits):
                    tok_copy(way, 1, p).start()

    def tok_relay(d, close, p):
        for way in (0, 1):
            here = lax.rem(rank, 2) == (1 - way if close else way)

            @pl.when(jnp.logical_and(held(way, d), here))
            def _():
                tok_landed(way, d, p).wait_recv()
                tok_pass(way, d, p, core).start()

            if d < split - 1:

                @pl.when(jnp.logical_and(onward(way, d), here))
                def _():
                    tok_copy(way, d + 1, p).start()

    def tok_ready(d, close):
        for way in (0, 1):
            here = lax.rem(rank, 2) == (1 - way if close else way)

            @pl.when(jnp.logical_and(held(way, d), here))
            def _():
                for p in range(bits):
                    tok_pass(way, d, p, 1 - core).wait_recv()

    chunks, _, chunk = ff_s.shape[1:]
    across = (((1,), (1,)), ((), ()))

    def target(i):
        t = (1 + inner, 2 - 2 * inner, 3, inner)[i]
        return t + side * (split - 1 - 2 * t)

    per = chunks // split

    def col(j, back=False):
        t = split - 1 - j // per if back else j // per
        return (t + side * (split - 1 - 2 * t)) * per + j % per

    def near(j):
        return away(j // per) * per + j % per

    def hid(i):
        tokens = tok_s[target(i)]
        gate = lax.dot_general(tokens, wide_s[0], across, preferred_element_type=f32)
        up = lax.dot_general(tokens, wide_s[1], across, preferred_element_type=f32)
        hid_s[i] = (gate / (1.0 + jnp.exp(-gate)) * up).astype(bf16)

    def offer(i, js):
        js = list(js)
        for at in range(len(js) + 1):
            if at < len(js):
                part(i, near(js[at]))
            if at:
                lead(i, near(js[at - 1]))

    def tp_copy(i, q):
        return remote(
            ff_s.at[i, q, other, :], tp_s.at[i, q], as_sem.at[i, q], ar_sem.at[i, q],
            {"tp": 1 - core},
        )

    def part(i, q):
        cols = pl.ds(pl.multiple_of(q * chunk, chunk), chunk)
        ff_s[i, q] = jnp.dot(
            hid_s[i], wide_s[2, :, cols], preferred_element_type=f32
        ).astype(bf16)
        tp_copy(i, q).start()

    def sum_copy(a, slot, q, to):
        return remote(
            red_s.at[a, q], rz_s.at[slot, q], ks_sem.at[a, q], kr_sem.at[slot, q],
            {"sp": to * plane + spot},
        )

    def pair(i, q):
        tp_copy(i, q).wait()
        return ff_s[i, q, mine, :].astype(f32) + tp_s[i, q].astype(f32)

    def summed(i, slots, q):
        mixed = pair(i, q)
        for slot in slots:
            sum_copy(0, slot, q, mate).wait_recv()
            mixed = mixed + rz_s[slot, q].astype(f32)
        return mixed

    def lead(i, q):
        red_s[i, q] = summed(i, (), q).astype(bf16)
        sum_copy(i, i, q, mate).start()

    follow = ((0, 1, 3), (2, 2, 4), (1, 4, 3))

    def trail(a, q):
        i, slot, out_slot = follow[a]
        red_s[a, q] = summed(i, (slot,), q).astype(bf16)
        sum_copy(a, out_slot, q, ahead if a < 2 else mate).start()

    def out_copy(q):
        view = out_ref.at[mine, pl.ds(pl.multiple_of(q * chunk, chunk), chunk)]
        return remote(view, view, os_sem.at[q], or_sem.at[q], {"tp": 1 - core})

    def out_landed(q):
        view = out_ref.at[other, pl.ds(pl.multiple_of(q * chunk, chunk), chunk)]
        return remote(view, view, os_sem.at[q], or_sem.at[q], {"tp": 1 - core})

    def finish(role, q):
        cols = pl.ds(pl.multiple_of(q * chunk, chunk), chunk)
        total = summed(split - 1, (0, 3) if role else (3,), q)
        out_ref[mine, cols] = (mid_s[mine, cols].astype(f32) + total).astype(bf16)
        out_copy(q).start()

    first = range(2 * per)
    second = range(2 * per, chunks)

    tok_start()
    relay(0, 3)

    @pl.when(inner == 0)
    def _():
        relay(1, 1)

    spread(1, 2)

    @pl.when(inner == 1)
    def _():
        relay(1, 1)

    spread(1, 3)

    @pl.when(inner == 0)
    def outer_plane():
        relay(1, 2)
        relay(1, 3)
        spread(2, 1)
        spread(2, 2)
        for p in range(bits):
            tok_relay(1, True, p)
        for c in (0, 1):
            for k in range(split):
                settle(c, k)
        tok_ready(1, True)
        hid(0)
        settle(2, 0)
        for j in range(per):
            part(0, near(j))
        relay(2, 1)
        for j in range(per):
            lead(0, near(j))
        spread(2, 3)
        settle(2, 1)
        offer(0, range(per, 2 * per))
        relay(2, 2)
        relay(2, 3)
        for p in range(bits):
            tok_relay(2, True, p)
        tok_ready(2, True)
        hid(1)
        offer(1, first)
        settle(2, 2)
        offer(1, range(2 * per, 3 * per))
        settle(2, 3)
        offer(1, range(3 * per, chunks))
        offer(0, range(2 * per, 3 * per))
        for j in range(3 * per, chunks):
            part(0, near(j))
        for p in range(bits):
            tok_relay(3, True, p)
        tok_ready(3, True)
        hid(2)
        offer(2, range(chunks))
        for j in range(3 * per, chunks):
            lead(0, near(j))
        hid(3)
        for j in range(chunks):
            part(3, near(j))
        for j in range(chunks):
            finish(0, col(j, True))

    @pl.when(inner == 1)
    def inner_plane():
        relay(1, 2)
        spread(2, 1)
        relay(1, 3)
        spread(2, 2)
        tok_relay(1, False, 0)
        for p in range(bits // 2):
            tok_relay(1, True, p)
        relay(2, 1)
        for p in range(1, bits - 1):
            tok_relay(1, False, p)
        for p in range(bits // 2, bits):
            tok_relay(1, True, p)
        for c in (0, 1):
            for k in range(split):
                settle(c, k)
        tok_relay(1, False, bits - 1)
        spread(2, 3)
        relay(2, 2)
        tok_ready(1, True)
        tok_ready(1, False)
        hid(0)
        tok_relay(2, False, 0)
        relay(2, 3)
        for p in range(1, bits - 1):
            tok_relay(2, False, p)
        hid(3)
        tok_relay(2, False, bits - 1)
        hid(1)
        for k in range(split):
            settle(2, k)
        for j in range(chunks):
            part(0, col(j))
        tok_ready(2, False)
        for j in range(chunks):
            part(1, col(j))
        hid(2)
        for j in range(chunks):
            part(2, col(j))
        for j in range(chunks):
            part(3, col(j))
        for j in range(chunks):
            trail(0, col(j))
        lag = chunks // 2
        for j in range(chunks + lag):
            if j < chunks:
                trail(1, col(j))
            if j >= lag:
                trail(2, col(j - lag, True))
        for j in range(chunks):
            finish(1, col(j))

    lax.fori_loop(1, n - me, state_sent, 0)
    for q in range(chunks):
        out_copy(q).wait_send()
        out_landed(q).wait_recv()
        for a in range(split - 1):
            sum_copy(a, a, q, mate).wait_send()
    for way in (0, 1):
        for d in range(1, split):

            @pl.when(onward(way, d - 1))
            def _():
                for p in range(bits):
                    tok_copy(way, d, p).wait_send()

            @pl.when(held(way, d))
            def _():
                for p in range(bits):
                    tok_pass(way, d, p, core).wait_send()

    for c in range(kinds):
        for k in range(split):
            for m in (1, 2):
                pass_copy(c, k, m).wait_send()
                relay_copy(c, k, m).wait_send()
            if k:
                z_copy(c, k).wait_send()


def layer(n, split, x, bg, extra, taps, dp, wr, wa, ow, res, gain, gw, uw, dw):
    channels, length = x.shape
    groups = channels // LANES
    rows, width = res.shape
    depth, full = gw.shape
    span = full // split
    kinds = 3
    cut = 512
    pieces = width // cut
    chunk = width // 4
    chunks = width // chunk
    half = rows // 2
    vmem = pl.BlockSpec(memory_space=pltpu.VMEM)
    hbm = pl.BlockSpec(memory_space=pl.ANY)
    dma = pltpu.SemaphoreType.DMA
    bf16, f32 = jnp.bfloat16, jnp.float32
    buf = pltpu.VMEM
    return pl.pallas_call(
        functools.partial(layer_kernel, n, split),
        out_shape=pltpu.VMEM((rows, width), bf16),
        in_specs=[hbm, hbm, hbm, vmem, vmem, vmem, vmem, hbm, hbm, vmem, hbm, hbm, hbm],
        out_specs=vmem,
        scratch_shapes=[
            buf((channels, length), bf16),
            buf((channels, length), bf16),
            buf((channels, length), f32),
            buf((channels, width), bf16),
            buf((rows, width), bf16),
            buf((kinds, depth, full), bf16),
            buf((kinds, full, depth), bf16),
            buf((length + 8, channels), f32),
            buf((8, channels), f32),
            buf((groups, LANES, 2 * LANES), bf16),
            buf((groups, length, LANES), f32),
            buf((groups, length, LANES), f32),
            buf((groups, length // 8, LANES), f32),
            buf((groups, length // 8, LANES), f32),
            buf((groups, length, LANES), f32),
            buf((2 * groups, LANES), f32),
            buf((n - 1, 2 * groups, LANES), f32),
            buf((groups, LANES), f32),
            buf((length, channels), bf16),
            buf((pieces, rows, cut), bf16),
            buf((pieces, rows, cut), bf16),
            buf((rows, width), bf16),
            buf((split, rows, width), bf16),
            buf((kinds, span, width), bf16),
            buf((split, rows, span), bf16),
            buf((split, chunks, rows, chunk), bf16),
            buf((split, chunks, half, chunk), bf16),
            buf((split - 1, chunks, half, chunk), bf16),
            buf((5, chunks, half, chunk), bf16),
            dma((8,)),
            dma,
            dma,
            dma((n - 1,)),
            dma((n - 1,)),
            dma((kinds, split - 1)),
            dma((kinds, split - 1)),
            dma((1,)),
            dma((1,)),
            dma((kinds, split, 2)),
            dma((kinds, split, 2)),
            dma((kinds, split, 2)),
            dma((kinds, split, 2)),
            dma((pieces,)),
            dma((pieces,)),
            dma((2, split - 1, 4)),
            dma((2, split - 1, 4)),
            dma((2, split - 1, 4)),
            dma((2, split - 1, 4)),
            dma((split, chunks)),
            dma((split, chunks)),
            dma((split - 1, chunks)),
            dma((5, chunks)),
            dma((chunks,)),
            dma((chunks,)),
        ],
        compiler_params=pltpu.CompilerParams(
            collective_id=1, has_side_effects=True, vmem_limit_bytes=54 << 20
        ),
        name="layer",
    )(x, bg, extra, taps, dp, wr, wa, ow, res, gain, gw, uw, dw)


def on_device(
    residual_in,
    mixer_input,
    branch_gate,
    conv_taps,
    recur_weight,
    admit_weight,
    decay_param,
    decay_extra,
    out_weight,
    norm_gain,
    gate_weight,
    up_weight,
    down_weight,
):
    n = lax.axis_size("sp")
    length = mixer_input.shape[1]
    width, share_ff = residual_in.shape[1], gate_weight.shape[1]
    split = 4
    depth = gate_weight.shape[0]
    if (
        lax.axis_size("tp") == 2
        and n == 4 * split
        and depth == LANES
        and width == n * depth
        and share_ff % LANES == 0
        and share_ff % (32 * split) == 0
        and 2 * recur_weight.shape[1] == LANES
        and conv_taps.shape[1] <= 9
        and residual_in.shape[0] == length
        and length % (2 * LANES) == 0
    ):
        return layer(
            n,
            split,
            mixer_input,
            branch_gate,
            decay_extra,
            conv_taps.T,
            decay_param.reshape(-1, LANES),
            recur_weight,
            admit_weight,
            out_weight,
            residual_in,
            norm_gain.reshape(-1, LANES),
            gate_weight,
            up_weight,
            down_weight,
        )
    halo = lax.ppermute(
        mixer_input[:, length - LANES :], "sp", [(i, i + 1) for i in range(n - 1)]
    )
    rate = -8.0 * jax.nn.softplus(-decay_param)[:, None]
    mixed_out = mixer(
        n,
        mixer_input,
        halo,
        branch_gate,
        decay_extra,
        conv_taps.astype(jnp.float32),
        rate,
        recur_weight.transpose(0, 2, 1),
        admit_weight.transpose(0, 2, 1),
    )
    row_count = residual_in.shape[0]
    partial_value = lax.dot_general(
        mixed_out, out_weight, (((0,), (0,)), ((), ())), preferred_element_type=jnp.float32
    )
    branch = lax.psum(partial_value.astype(jnp.bfloat16), "tp").astype(jnp.float32)
    middle = (residual_in.astype(jnp.float32) + branch).astype(jnp.bfloat16)
    middle_wide = middle.astype(jnp.float32)
    row_scale = lax.rsqrt(jnp.mean(middle_wide * middle_wide, axis=1, keepdims=True) + 1e-06)
    normed = (middle_wide * row_scale * norm_gain.astype(jnp.float32)).astype(jnp.bfloat16)
    gate_pre = jnp.dot(
        normed,
        lax.all_gather(gate_weight, "sp", axis=0, tiled=True),
        preferred_element_type=jnp.float32,
    )
    up_pre = jnp.dot(
        normed,
        lax.all_gather(up_weight, "sp", axis=0, tiled=True),
        preferred_element_type=jnp.float32,
    )
    down_whole = lax.all_gather(down_weight, "sp", axis=0, tiled=True)
    hidden = (jax.nn.silu(gate_pre) * up_pre).astype(jnp.bfloat16)
    share = row_count // lax.axis_size("tp")
    channel_out = lax.psum_scatter(
        lax.dot_general(
            hidden, down_whole, (((1,), (1,)), ((), ())), preferred_element_type=jnp.float32
        ).astype(jnp.bfloat16),
        "tp",
        scatter_dimension=0,
        tiled=True,
    ).astype(jnp.float32)
    first_row = lax.axis_index("tp") * share
    own_rows = lax.dynamic_slice_in_dim(middle, first_row, share, 0)
    layer_rows = (own_rows.astype(jnp.float32) + channel_out).astype(jnp.bfloat16)
    return lax.all_gather(layer_rows, "tp", axis=0, tiled=True)


def solution(mesh):
    placed = (
        P("sp", None),
        P("tp", "sp"),
        P("tp", "sp"),
        P("tp", None),
        P("tp", None, None),
        P("tp", None, None),
        P("tp"),
        P("tp", "sp"),
        P("tp", None),
        P(),
        P("sp", "tp"),
        P("sp", "tp"),
        P("sp", "tp"),
    )
    return jax.shard_map(
        on_device, mesh=mesh, in_specs=placed, out_specs=P("sp", None), check_vma=False
    )
```

```python
import functools

import jax
import jax.numpy as jnp
from jax import lax
from jax.experimental import pallas as pl
from jax.experimental.pallas import tpu as pltpu
from jax.sharding import PartitionSpec as P

MESH = pl.DeviceIdType.MESH
LANES = 128


def neg_expm1(v):
    series = jnp.full_like(v, 1.0)
    for k in range(9, 1, -1):
        series = 1.0 + series * v * (1.0 / k)
    return jnp.where(v > -0.5, -v * series, 1.0 - jnp.exp(v))


def mixer_kernel(
    n,
    x_ref,
    halo_ref,
    bg_ref,
    extra_ref,
    taps_ref,
    rate_ref,
    wr_ref,
    wa_ref,
    out_ref,
    state_s,
    run_s,
    ends_s,
    all_s,
    in_s,
    send_sem,
    recv_sem,
):
    me = lax.axis_index("sp")
    barrier = pltpu.get_barrier_semaphore()

    def greet(k, carry):
        pl.semaphore_signal(
            barrier, inc=1, device_id={"sp": lax.rem(me + k, n)}, device_id_type=MESH
        )
        return carry

    lax.fori_loop(1, n, greet, 0)
    channels, length = x_ref.shape
    block = wr_ref.shape[1]
    groups = channels // LANES
    tap_count = taps_ref.shape[1]
    lane = lax.broadcasted_iota(jnp.int32, (LANES, length), 1)

    def local(g, carry):
        rows = pl.ds(pl.multiple_of(g * LANES, LANES), LANES)
        wide = jnp.concatenate(
            [halo_ref[rows, :].astype(jnp.float32), x_ref[rows, :].astype(jnp.float32)], axis=1
        )
        taps = taps_ref[rows, :]
        total = taps[:, tap_count - 1 :] * wide[:, LANES:]
        for tap in range(tap_count - 2, -1, -1):
            total = total + taps[:, tap : tap + 1] * pltpu.roll(wide, tap_count - 1 - tap, 1)[:, LANES:]
        conv = total.astype(jnp.bfloat16)
        per = LANES // block
        recur, admit = [], []
        for b in range(per):
            part = conv[b * block : (b + 1) * block]
            recur.append(jnp.dot(wr_ref[g * per + b], part, preferred_element_type=jnp.float32))
            admit.append(jnp.dot(wa_ref[g * per + b], part, preferred_element_type=jnp.float32))
        recur = jax.nn.sigmoid(jnp.concatenate(recur, axis=0))
        admit = jax.nn.sigmoid(jnp.concatenate(admit, axis=0))
        log_decay = recur * rate_ref[rows, :] + extra_ref[rows, :]
        a = jnp.exp(log_decay)
        b = jnp.sqrt(neg_expm1(2.0 * log_decay)) * admit * conv.astype(jnp.float32)
        shift = 1
        while shift < length:
            seen = lane >= shift
            b = b + a * jnp.where(seen, pltpu.roll(b, shift, 1), 0.0)
            a = a * jnp.where(seen, pltpu.roll(a, shift, 1), 1.0)
            shift *= 2
        state_s[rows, :] = b
        run_s[rows, :] = a
        ends_s[pl.ds(g, 1), :] = a[:, length - LANES :].T[LANES - 1 :]
        ends_s[pl.ds(groups + g, 1), :] = b[:, length - LANES :].T[LANES - 1 :]
        return carry

    lax.fori_loop(0, groups, local, 0)
    pl.semaphore_wait(barrier, n - 1)

    def copy_to(k):
        return pltpu.make_async_remote_copy(
            src_ref=ends_s,
            dst_ref=all_s.at[k - 1],
            send_sem=send_sem.at[k - 1],
            recv_sem=recv_sem.at[k - 1],
            device_id={"sp": lax.rem(me + k, n)},
            device_id_type=MESH,
        )

    def send(k, carry):
        copy_to(k).start()
        return carry

    lax.fori_loop(1, n, send, 0)

    def finish(k, carry):
        copy_to(k).wait()
        return carry

    lax.fori_loop(1, n, finish, 0)

    def fold(i, before):
        k = n - 1 - i
        part = all_s[k - 1]
        new = part[:groups] * before + part[groups:]
        return jnp.where(k <= me, new, before)

    in_s[...] = lax.fori_loop(0, n - 1, fold, jnp.zeros((groups, LANES), jnp.float32))

    def close(g, carry):
        rows = pl.ds(pl.multiple_of(g * LANES, LANES), LANES)
        entering = jnp.broadcast_to(in_s[pl.ds(g, 1), :], (LANES, LANES)).T
        entering = jnp.concatenate([entering] * (length // LANES), axis=1)
        states = state_s[rows, :] + run_s[rows, :] * entering
        v = bg_ref[rows, :].astype(jnp.float32)
        act = 0.5 * v * (1.0 + jnp.tanh(0.7978845608028654 * (v + 0.044715 * v * v * v)))
        out_ref[rows, :] = (states * act).astype(jnp.bfloat16)
        return carry

    lax.fori_loop(0, groups, close, 0)


def mixer(n, x, halo, bg, extra, taps, rate, wr, wa):
    channels, length = x.shape
    groups = channels // LANES
    vmem = pl.BlockSpec(memory_space=pltpu.VMEM)
    return pl.pallas_call(
        functools.partial(mixer_kernel, n),
        out_shape=jax.ShapeDtypeStruct((channels, length), jnp.bfloat16),
        in_specs=[vmem] * 8,
        out_specs=vmem,
        scratch_shapes=[
            pltpu.VMEM((channels, length), jnp.float32),
            pltpu.VMEM((channels, length), jnp.float32),
            pltpu.VMEM((2 * groups, LANES), jnp.float32),
            pltpu.VMEM((n - 1, 2 * groups, LANES), jnp.float32),
            pltpu.VMEM((groups, LANES), jnp.float32),
            pltpu.SemaphoreType.DMA((n - 1,)),
            pltpu.SemaphoreType.DMA((n - 1,)),
        ],
        compiler_params=pltpu.CompilerParams(
            collective_id=0, has_side_effects=True, vmem_limit_bytes=24 << 20
        ),
        cost_estimate=pl.CostEstimate(
            flops=200 * channels * length, bytes_accessed=12 * channels * length, transcendentals=0
        ),
        name="mixer",
    )(x, halo, bg, extra, taps, rate, wr, wa)


def layer_kernel(
    n, split,
    x_ref, bg_ref, extra_ref, taps_ref, dp_ref, wr_ref, wa_ref, ow_ref, res_ref, gain_ref,
    gw_ref, uw_ref, dw_ref,
    out_ref,
    x_s, bg_s, extra_s, ow_s, res_s, raw_s, pack_s,
    xt_s, halo_s, wbd_s, a_s, b_s, ea_s, eb_s, act_s, ends_s, all_s, in_s, mix_s,
    part_s, part_r, mid_s, tok_s, wide_s, hid_s, ff_s, tp_s, red_s, rz_s,
    in_sem, hs_sem, hr_sem, ss_sem, sr_sem,
    zs_sem, zr_sem, ps_sem, pr_sem, fs_sem, fr_sem, rs_sem, rr_sem,
    bs_sem, br_sem, ts_sem, tr_sem, cs_sem, cr_sem,
    as_sem, ar_sem, ks_sem, kr_sem, os_sem, or_sem,
):
    me = lax.axis_index("sp")
    core = lax.axis_index("tp")
    plane = n // split
    rank, spot = me // plane, lax.rem(me, plane)
    f32, bf16 = jnp.float32, jnp.bfloat16
    channels, length = x_s.shape
    groups = channels // LANES
    block = wr_ref.shape[1]
    taps = taps_ref.shape[0]
    kinds, full, depth = pack_s.shape
    span = full // split
    width = mid_s.shape[1]
    barrier = pltpu.get_barrier_semaphore()

    raw_refs = (gw_ref, uw_ref, dw_ref)
    loads = [
        pltpu.make_async_copy(src, dst, in_sem.at[i])
        for i, (src, dst) in enumerate(
            [
                (x_ref, x_s),
                (gw_ref, raw_s.at[0]),
                (uw_ref, raw_s.at[1]),
                (dw_ref, raw_s.at[2]),
                (extra_ref, extra_s),
                (bg_ref, bg_s),
                (ow_ref, ow_s),
                (res_ref, res_s),
            ]
        )
    ]
    for load in loads:
        load.start()

    def greet(k, carry):
        pl.semaphore_signal(
            barrier, inc=1, device_id={"sp": lax.rem(me + k, n)}, device_id_type=MESH
        )
        return carry

    lax.fori_loop(1, n, greet, 0)
    pl.semaphore_signal(barrier, inc=1, device_id={"tp": 1 - core}, device_id_type=MESH)

    def remote(src, dst, ssem, rsem, where):
        return pltpu.make_async_remote_copy(
            src_ref=src, dst_ref=dst, send_sem=ssem, recv_sem=rsem,
            device_id=where, device_id_type=MESH,
        )

    def lanes(i):
        return pl.ds(pl.multiple_of(i * LANES, LANES), LANES)

    def own(c):
        return pack_s.at[c, pl.ds(pl.multiple_of(rank * span, span), span)]

    def window(c, source):
        return wide_s.at[c, :, lanes(source)]

    side = rank // 2
    inner = lax.rem(rank, 2) + side - 2 * lax.rem(rank, 2) * side
    mate = rank + 1 - 2 * lax.rem(rank, 2)
    ahead = rank + 1 - 2 * side

    def away(k):
        if k < 2:
            return (rank, mate)[k]
        t = 2 if k == 2 else 3
        return t + side * (split - 1 - 2 * t)

    def there(k):
        return k if k < 2 else 3 - inner

    def z_copy(c, k):
        to = away(k)
        return remote(
            pack_s.at[c, pl.ds(pl.multiple_of(to * span, span), span)], window(c, me),
            zs_sem.at[c, k - 1], zr_sem.at[c, there(k) - 1], {"sp": to * plane + spot},
        )

    def z_landed(c, k):
        source = away(k) * plane + spot
        return remote(
            own(c), window(c, source), zs_sem.at[c, k - 1], zr_sem.at[c, k - 1], {"sp": source}
        )

    def beside(m):
        return spot + 1 - 2 * lax.rem(spot, 2) if m == 1 else spot + 2 - 4 * (spot // 2)

    def pass_copy(c, k, m):
        source = away(k) * plane + spot
        return remote(
            window(c, source) if k else own(c), window(c, source),
            fs_sem.at[c, k, m - 1], fr_sem.at[c, k, m - 1], {"sp": rank * plane + beside(m)},
        )

    def pass_landed(c, k, m):
        source = away(k) * plane + beside(m)
        return remote(
            window(c, source), window(c, source),
            fs_sem.at[c, k, m - 1], fr_sem.at[c, k, m - 1], {"sp": rank * plane + beside(m)},
        )

    def relay_window(c, k, m, where):
        source = away(k) * plane + where
        return wide_s.at[c, pl.ds((m - 1) * (span // 2), span // 2), lanes(source)]

    def relay_copy(c, k, m):
        view = relay_window(c, k, m, beside(m))
        return remote(
            view, view, rs_sem.at[c, k, m - 1], rr_sem.at[c, k, m - 1],
            {"sp": rank * plane + beside(3 - m)},
        )

    def relay_landed(c, k, m):
        view = relay_window(c, k, m, 3 - spot)
        return remote(
            view, view, rs_sem.at[c, k, m - 1], rr_sem.at[c, k, m - 1],
            {"sp": rank * plane + beside(3 - m)},
        )

    def z_start(c):
        @pl.when(inner == 0)
        def _():
            z_copy(c, 1).start()

        for k in range(2, split):
            z_copy(c, k).start()

    def z_mate(c):
        @pl.when(inner == 1)
        def _():
            z_copy(c, 1).start()

    def spread(c, k):
        if k:
            z_landed(c, k).wait_recv()
        for m in (1, 2):
            pass_copy(c, k, m).start()

    def relay(c, k):
        for m in (1, 2):
            pass_landed(c, k, m).wait_recv()
            relay_copy(c, k, m).start()

    def settle(c, k):
        for m in (1, 2):
            relay_landed(c, k, m).wait_recv()

    def turn(c):
        loads[1 + c].wait()

        def step(j, carry):
            pack_s[c, lanes(j), :] = raw_s[c, :, lanes(j)].T
            return carry

        lax.fori_loop(0, full // LANES, step, 0)

    def keep(c):
        wide_s[c, :, lanes(me)] = own(c)[...]

    loads[0].wait()

    def flip(g, carry):
        xt_s[pl.ds(8, length), lanes(g)] = x_s[lanes(g), :].astype(f32).T
        return carry

    lax.fori_loop(0, groups, flip, 0)
    turn(0)
    pl.semaphore_wait(barrier, n)
    halo = remote(
        xt_s.at[pl.ds(length, 8), :], halo_s, hs_sem, hr_sem, {"sp": lax.rem(me + 1, n)}
    )
    halo.start()
    z_mate(0)
    z_start(0)
    spread(0, 0)
    turn(1)
    spread(1, 0)
    turn(2)
    for c in range(kinds):
        keep(c)

    rowb = lax.broadcasted_iota(jnp.int32, (LANES, LANES), 0) // block
    colb = lax.broadcasted_iota(jnp.int32, (LANES, LANES), 1) // block
    eye_r = lax.broadcasted_iota(jnp.int32, (block, LANES), 0)
    eye_c = lax.rem(lax.broadcasted_iota(jnp.int32, (block, LANES), 1), block)
    twice = jnp.where(eye_r == eye_c, 1.0, 0.0).astype(bf16)

    def widen(g, carry):
        for slot, w_ref in ((0, wr_ref), (1, wa_ref)):
            pair = jnp.concatenate([w_ref[2 * g], w_ref[2 * g + 1]], axis=0)
            both = jnp.dot(pair, twice, preferred_element_type=f32)
            wbd_s[g, :, slot * LANES : (slot + 1) * LANES] = jnp.where(
                rowb == colb, both, 0.0
            ).astype(bf16)
        return carry

    lax.fori_loop(0, groups, widen, 0)
    loads[4].wait()
    halo.wait()
    xt_s[0:8, :] = halo_s[...] * jnp.where(me > 0, 1.0, 0.0)

    octets = length // 8
    sub = lax.broadcasted_iota(jnp.int32, (octets, 8, LANES), 1)
    row = lax.broadcasted_iota(jnp.int32, (octets, LANES), 0)

    def local(g, carry):
        cols = lanes(g)
        tap = taps_ref[:, cols].astype(f32)
        total = tap[taps - 1 : taps] * xt_s[pl.ds(8, length), cols]
        for k in range(taps - 2, -1, -1):
            total = total + tap[k : k + 1] * xt_s[pl.ds(9 - taps + k, length), cols]
        conv = total.astype(bf16)
        both = jnp.dot(conv, wbd_s[g], preferred_element_type=f32)
        recur = jax.nn.sigmoid(both[:, :LANES])
        admit = jax.nn.sigmoid(both[:, LANES:])
        rate = -8.0 * jax.nn.softplus(-dp_ref[pl.ds(g, 1), :])
        log_decay = recur * rate + extra_s[lanes(g), :].T
        a = jnp.exp(log_decay)
        b = jnp.sqrt(neg_expm1(2.0 * log_decay)) * admit * conv.astype(f32)
        a = a.reshape(octets, 8, LANES)
        b = b.reshape(octets, 8, LANES)
        for shift in (1, 2, 4):
            seen = sub >= shift
            b = b + a * jnp.where(seen, pltpu.roll(b, shift, 1), 0.0)
            a = a * jnp.where(seen, pltpu.roll(a, shift, 1), 1.0)
        a_s[g] = a.reshape(length, LANES)
        b_s[g] = b.reshape(length, LANES)
        ea = a_s[g, pl.ds(7, octets, stride=8), :]
        eb = b_s[g, pl.ds(7, octets, stride=8), :]
        shift = 1
        while shift < octets:
            seen = row >= shift
            eb = eb + ea * jnp.where(seen, pltpu.roll(eb, shift, 0), 0.0)
            ea = ea * jnp.where(seen, pltpu.roll(ea, shift, 0), 1.0)
            shift *= 2
        ends_s[pl.ds(g, 1), :] = ea[octets - 1 :]
        ends_s[pl.ds(groups + g, 1), :] = eb[octets - 1 :]
        ea_s[g] = jnp.where(row >= 1, pltpu.roll(ea, 1, 0), 1.0)
        eb_s[g] = jnp.where(row >= 1, pltpu.roll(eb, 1, 0), 0.0)
        return carry

    lax.fori_loop(0, groups, local, 0)

    def state(k):
        return remote(
            ends_s, all_s.at[k - 1], ss_sem.at[k - 1], sr_sem.at[k - 1],
            {"sp": lax.rem(me + k, n)},
        )

    def state_send(k, carry):
        state(k).start()
        return carry

    lax.fori_loop(1, n - me, state_send, 0)
    z_start(1)
    spread(0, 1)
    relay(0, 0)
    spread(2, 0)
    loads[5].wait()

    def gelu(g, carry):
        v = bg_s[lanes(g), :].astype(f32).T
        act_s[g] = 0.5 * v * (1.0 + jnp.tanh(0.7978845608028654 * (v + 0.044715 * v * v * v)))
        return carry

    lax.fori_loop(0, groups, gelu, 0)
    relay(1, 0)
    z_mate(1)
    spread(0, 2)
    relay(0, 1)
    spread(0, 3)
    relay(2, 0)
    z_mate(2)
    spread(1, 1)

    def state_wait(k, carry):
        remote(
            ends_s, all_s.at[k - 1], ss_sem.at[k - 1], sr_sem.at[k - 1],
            {"sp": lax.rem(me - k + n, n)},
        ).wait_recv()
        return carry

    lax.fori_loop(1, me + 1, state_wait, 0)

    def state_sent(k, carry):
        state(k).wait_send()
        return carry

    def fold(i, before):
        part = all_s[me - 1 - i]
        return part[:groups] * before + part[groups:]

    in_s[...] = lax.fori_loop(0, me, fold, jnp.zeros((groups, LANES), f32))

    def close(g, carry):
        enter = eb_s[g] + ea_s[g] * in_s[pl.ds(g, 1), :]
        states = jnp.concatenate(
            [
                b_s[g, i * 8 : i * 8 + 8, :] + a_s[g, i * 8 : i * 8 + 8, :] * enter[i : i + 1]
                for i in range(octets)
            ],
            axis=0,
        )
        mix_s[:, lanes(g)] = (states * act_s[g]).astype(bf16)
        return carry

    lax.fori_loop(0, groups, close, 0)

    pieces, row_count, cut = part_s.shape

    def swap(i):
        return remote(
            part_s.at[i], part_r.at[i], bs_sem.at[i], br_sem.at[i], {"tp": 1 - core}
        )

    loads[6].wait()
    for i in range(pieces):
        part_s[i] = jnp.dot(
            mix_s[...], ow_s[:, i * cut : (i + 1) * cut], preferred_element_type=f32
        ).astype(bf16)
        swap(i).start()
    z_start(2)
    relay(0, 2)
    loads[7].wait()
    square = jnp.zeros((row_count, 1), f32)
    for i in range(pieces):
        swap(i).wait()
        cols = slice(i * cut, (i + 1) * cut)
        branch = part_s[i].astype(f32) + part_r[i].astype(f32)
        middle = (res_s[:, cols].astype(f32) + branch).astype(bf16)
        mid_s[:, cols] = middle
        middle = middle.astype(f32)
        square = square + jnp.sum(middle * middle, axis=1, keepdims=True)
    scale = lax.rsqrt(square * (1.0 / (pieces * cut)) + 1e-06)
    for i in range(width // LANES):
        cols = slice(i * LANES, (i + 1) * LANES)
        gain = gain_ref[i : i + 1, :].astype(f32)
        tok_s[rank, :, cols] = (mid_s[:, cols].astype(f32) * scale * gain).astype(bf16)

    half = row_count // 2
    mine = pl.ds(pl.multiple_of(core * half, half), half)
    other = pl.ds(pl.multiple_of((1 - core) * half, half), half)

    bits = ts_sem.shape[2]
    bit = half // bits

    def some(which, p):
        return pl.ds(pl.multiple_of(which * half + p * bit, bit), bit)

    def tok_copy(way, d, p):
        step = 1 - 2 * way
        view = tok_s.at[rank - (d - 1) * step, some(core, p), :]
        return remote(
            view, view, ts_sem.at[way, d - 1, p], tr_sem.at[way, d - 1, p],
            {"sp": (rank + step) * plane + spot},
        )

    def tok_landed(way, d, p):
        step = 1 - 2 * way
        view = tok_s.at[rank - d * step, some(core, p), :]
        return remote(
            view, view, ts_sem.at[way, d - 1, p], tr_sem.at[way, d - 1, p],
            {"sp": (rank - step) * plane + spot},
        )

    def tok_pass(way, d, p, which):
        view = tok_s.at[rank - d * (1 - 2 * way), some(which, p), :]
        return remote(
            view, view, cs_sem.at[way, d - 1, p], cr_sem.at[way, d - 1, p], {"tp": 1 - core}
        )

    def held(way, d):
        return rank >= d if way == 0 else rank <= split - 1 - d

    def onward(way, d):
        return (
            jnp.logical_and(rank >= d, rank < split - 1)
            if way == 0
            else jnp.logical_and(rank <= split - 1 - d, rank > 0)
        )

    def tok_start():
        for way in (0, 1):

            @pl.when(onward(way, 0))
            def _():
                for p in range(bits):
                    tok_copy(way, 1, p).start()

    def tok_relay(d, close, p):
        for way in (0, 1):
            here = lax.rem(rank, 2) == (1 - way if close else way)

            @pl.when(jnp.logical_and(held(way, d), here))
            def _():
                tok_landed(way, d, p).wait_recv()
                tok_pass(way, d, p, core).start()

            if d < split - 1:

                @pl.when(jnp.logical_and(onward(way, d), here))
                def _():
                    tok_copy(way, d + 1, p).start()

    def tok_ready(d, close):
        for way in (0, 1):
            here = lax.rem(rank, 2) == (1 - way if close else way)

            @pl.when(jnp.logical_and(held(way, d), here))
            def _():
                for p in range(bits):
                    tok_pass(way, d, p, 1 - core).wait_recv()

    chunks, _, chunk = ff_s.shape[1:]
    across = (((1,), (1,)), ((), ()))

    def target(i):
        t = (1 + inner, 2 - 2 * inner, 3, inner)[i]
        return t + side * (split - 1 - 2 * t)

    per = chunks // split

    def col(j, back=False):
        t = split - 1 - j // per if back else j // per
        return (t + side * (split - 1 - 2 * t)) * per + j % per

    def near(j):
        return away(j // per) * per + j % per

    def hid(i):
        tokens = tok_s[target(i)]
        gate = lax.dot_general(tokens, wide_s[0], across, preferred_element_type=f32)
        up = lax.dot_general(tokens, wide_s[1], across, preferred_element_type=f32)
        hid_s[i] = (gate / (1.0 + jnp.exp(-gate)) * up).astype(bf16)

    def offer(i, js):
        js = list(js)
        for at in range(len(js) + 1):
            if at < len(js):
                part(i, near(js[at]))
            if at:
                lead(i, near(js[at - 1]))

    def tp_copy(i, q):
        return remote(
            ff_s.at[i, q, other, :], tp_s.at[i, q], as_sem.at[i, q], ar_sem.at[i, q],
            {"tp": 1 - core},
        )

    def part(i, q):
        cols = pl.ds(pl.multiple_of(q * chunk, chunk), chunk)
        ff_s[i, q] = jnp.dot(
            hid_s[i], wide_s[2, :, cols], preferred_element_type=f32
        ).astype(bf16)
        tp_copy(i, q).start()

    def sum_copy(a, slot, q, to):
        return remote(
            red_s.at[a, q], rz_s.at[slot, q], ks_sem.at[a, q], kr_sem.at[slot, q],
            {"sp": to * plane + spot},
        )

    def pair(i, q):
        tp_copy(i, q).wait()
        return ff_s[i, q, mine, :].astype(f32) + tp_s[i, q].astype(f32)

    def summed(i, slots, q):
        mixed = pair(i, q)
        for slot in slots:
            sum_copy(0, slot, q, mate).wait_recv()
            mixed = mixed + rz_s[slot, q].astype(f32)
        return mixed

    def lead(i, q):
        red_s[i, q] = summed(i, (), q).astype(bf16)
        sum_copy(i, i, q, mate).start()

    follow = ((0, 1, 3), (2, 2, 4), (1, 4, 3))

    def trail(a, q):
        i, slot, out_slot = follow[a]
        red_s[a, q] = summed(i, (slot,), q).astype(bf16)
        sum_copy(a, out_slot, q, ahead if a < 2 else mate).start()

    def out_copy(q):
        view = out_ref.at[mine, pl.ds(pl.multiple_of(q * chunk, chunk), chunk)]
        return remote(view, view, os_sem.at[q], or_sem.at[q], {"tp": 1 - core})

    def out_landed(q):
        view = out_ref.at[other, pl.ds(pl.multiple_of(q * chunk, chunk), chunk)]
        return remote(view, view, os_sem.at[q], or_sem.at[q], {"tp": 1 - core})

    def finish(role, q):
        cols = pl.ds(pl.multiple_of(q * chunk, chunk), chunk)
        total = summed(split - 1, (0, 3) if role else (3,), q)
        out_ref[mine, cols] = (mid_s[mine, cols].astype(f32) + total).astype(bf16)
        out_copy(q).start()

    first = range(2 * per)
    second = range(2 * per, chunks)

    tok_start()
    relay(0, 3)

    @pl.when(inner == 0)
    def _():
        relay(1, 1)

    spread(1, 2)

    @pl.when(inner == 1)
    def _():
        relay(1, 1)

    spread(1, 3)

    @pl.when(inner == 0)
    def outer_plane():
        relay(1, 2)
        relay(1, 3)
        spread(2, 1)
        spread(2, 2)
        for p in range(bits):
            tok_relay(1, True, p)
        for c in (0, 1):
            for k in range(split):
                settle(c, k)
        tok_ready(1, True)
        hid(0)
        settle(2, 0)
        for j in range(per):
            part(0, near(j))
        relay(2, 1)
        for j in range(per):
            lead(0, near(j))
        spread(2, 3)
        settle(2, 1)
        offer(0, range(per, 2 * per))
        relay(2, 2)
        relay(2, 3)
        for p in range(bits):
            tok_relay(2, True, p)
        tok_ready(2, True)
        hid(1)
        offer(1, first)
        settle(2, 2)
        offer(1, range(2 * per, 3 * per))
        settle(2, 3)
        offer(1, range(3 * per, chunks))
        for j in second:
            part(0, near(j))
        for p in range(bits):
            tok_relay(3, True, p)
        tok_ready(3, True)
        hid(2)
        offer(2, range(chunks))
        for j in second:
            lead(0, near(j))
        hid(3)
        for j in range(chunks):
            part(3, near(j))
        for j in range(chunks):
            finish(0, col(j, True))

    @pl.when(inner == 1)
    def inner_plane():
        relay(1, 2)
        spread(2, 1)
        relay(1, 3)
        spread(2, 2)
        tok_relay(1, False, 0)
        for p in range(bits // 2):
            tok_relay(1, True, p)
        relay(2, 1)
        for p in range(1, bits - 1):
            tok_relay(1, False, p)
        for p in range(bits // 2, bits):
            tok_relay(1, True, p)
        for c in (0, 1):
            for k in range(split):
                settle(c, k)
        tok_relay(1, False, bits - 1)
        spread(2, 3)
        relay(2, 2)
        tok_ready(1, True)
        tok_ready(1, False)
        hid(0)
        tok_relay(2, False, 0)
        relay(2, 3)
        for p in range(1, bits - 1):
            tok_relay(2, False, p)
        hid(3)
        tok_relay(2, False, bits - 1)
        hid(1)
        for k in range(split):
            settle(2, k)
        for j in range(chunks):
            part(0, col(j))
        tok_ready(2, False)
        for j in range(chunks):
            part(1, col(j))
        hid(2)
        for j in range(chunks):
            part(2, col(j))
        for j in range(chunks):
            part(3, col(j))
        for j in range(chunks):
            trail(0, col(j))
        lag = chunks // 2
        for j in range(chunks + lag):
            if j < chunks:
                trail(1, col(j))
            if j >= lag:
                trail(2, col(j - lag, True))
        for j in range(chunks):
            finish(1, col(j))

    lax.fori_loop(1, n - me, state_sent, 0)
    for q in range(chunks):
        out_copy(q).wait_send()
        out_landed(q).wait_recv()
        for a in range(split - 1):
            sum_copy(a, a, q, mate).wait_send()
    for way in (0, 1):
        for d in range(1, split):

            @pl.when(onward(way, d - 1))
            def _():
                for p in range(bits):
                    tok_copy(way, d, p).wait_send()

            @pl.when(held(way, d))
            def _():
                for p in range(bits):
                    tok_pass(way, d, p, core).wait_send()

    for c in range(kinds):
        for k in range(split):
            for m in (1, 2):
                pass_copy(c, k, m).wait_send()
                relay_copy(c, k, m).wait_send()
            if k:
                z_copy(c, k).wait_send()


def layer(n, split, x, bg, extra, taps, dp, wr, wa, ow, res, gain, gw, uw, dw):
    channels, length = x.shape
    groups = channels // LANES
    rows, width = res.shape
    depth, full = gw.shape
    span = full // split
    kinds = 3
    cut = 512
    pieces = width // cut
    chunk = width // 4
    chunks = width // chunk
    half = rows // 2
    vmem = pl.BlockSpec(memory_space=pltpu.VMEM)
    hbm = pl.BlockSpec(memory_space=pl.ANY)
    dma = pltpu.SemaphoreType.DMA
    bf16, f32 = jnp.bfloat16, jnp.float32
    buf = pltpu.VMEM
    return pl.pallas_call(
        functools.partial(layer_kernel, n, split),
        out_shape=pltpu.VMEM((rows, width), bf16),
        in_specs=[hbm, hbm, hbm, vmem, vmem, vmem, vmem, hbm, hbm, vmem, hbm, hbm, hbm],
        out_specs=vmem,
        scratch_shapes=[
            buf((channels, length), bf16),
            buf((channels, length), bf16),
            buf((channels, length), f32),
            buf((channels, width), bf16),
            buf((rows, width), bf16),
            buf((kinds, depth, full), bf16),
            buf((kinds, full, depth), bf16),
            buf((length + 8, channels), f32),
            buf((8, channels), f32),
            buf((groups, LANES, 2 * LANES), bf16),
            buf((groups, length, LANES), f32),
            buf((groups, length, LANES), f32),
            buf((groups, length // 8, LANES), f32),
            buf((groups, length // 8, LANES), f32),
            buf((groups, length, LANES), f32),
            buf((2 * groups, LANES), f32),
            buf((n - 1, 2 * groups, LANES), f32),
            buf((groups, LANES), f32),
            buf((length, channels), bf16),
            buf((pieces, rows, cut), bf16),
            buf((pieces, rows, cut), bf16),
            buf((rows, width), bf16),
            buf((split, rows, width), bf16),
            buf((kinds, span, width), bf16),
            buf((split, rows, span), bf16),
            buf((split, chunks, rows, chunk), bf16),
            buf((split, chunks, half, chunk), bf16),
            buf((split - 1, chunks, half, chunk), bf16),
            buf((5, chunks, half, chunk), bf16),
            dma((8,)),
            dma,
            dma,
            dma((n - 1,)),
            dma((n - 1,)),
            dma((kinds, split - 1)),
            dma((kinds, split - 1)),
            dma((1,)),
            dma((1,)),
            dma((kinds, split, 2)),
            dma((kinds, split, 2)),
            dma((kinds, split, 2)),
            dma((kinds, split, 2)),
            dma((pieces,)),
            dma((pieces,)),
            dma((2, split - 1, 4)),
            dma((2, split - 1, 4)),
            dma((2, split - 1, 4)),
            dma((2, split - 1, 4)),
            dma((split, chunks)),
            dma((split, chunks)),
            dma((split - 1, chunks)),
            dma((5, chunks)),
            dma((chunks,)),
            dma((chunks,)),
        ],
        compiler_params=pltpu.CompilerParams(
            collective_id=1, has_side_effects=True, vmem_limit_bytes=54 << 20
        ),
        name="layer",
    )(x, bg, extra, taps, dp, wr, wa, ow, res, gain, gw, uw, dw)


def on_device(
    residual_in,
    mixer_input,
    branch_gate,
    conv_taps,
    recur_weight,
    admit_weight,
    decay_param,
    decay_extra,
    out_weight,
    norm_gain,
    gate_weight,
    up_weight,
    down_weight,
):
    n = lax.axis_size("sp")
    length = mixer_input.shape[1]
    width, share_ff = residual_in.shape[1], gate_weight.shape[1]
    split = 4
    depth = gate_weight.shape[0]
    if (
        lax.axis_size("tp") == 2
        and n == 4 * split
        and depth == LANES
        and width == n * depth
        and share_ff % LANES == 0
        and share_ff % (32 * split) == 0
        and 2 * recur_weight.shape[1] == LANES
        and conv_taps.shape[1] <= 9
        and residual_in.shape[0] == length
        and length % (2 * LANES) == 0
    ):
        return layer(
            n,
            split,
            mixer_input,
            branch_gate,
            decay_extra,
            conv_taps.T,
            decay_param.reshape(-1, LANES),
            recur_weight,
            admit_weight,
            out_weight,
            residual_in,
            norm_gain.reshape(-1, LANES),
            gate_weight,
            up_weight,
            down_weight,
        )
    halo = lax.ppermute(
        mixer_input[:, length - LANES :], "sp", [(i, i + 1) for i in range(n - 1)]
    )
    rate = -8.0 * jax.nn.softplus(-decay_param)[:, None]
    mixed_out = mixer(
        n,
        mixer_input,
        halo,
        branch_gate,
        decay_extra,
        conv_taps.astype(jnp.float32),
        rate,
        recur_weight.transpose(0, 2, 1),
        admit_weight.transpose(0, 2, 1),
    )
    row_count = residual_in.shape[0]
    partial_value = lax.dot_general(
        mixed_out, out_weight, (((0,), (0,)), ((), ())), preferred_element_type=jnp.float32
    )
    branch = lax.psum(partial_value.astype(jnp.bfloat16), "tp").astype(jnp.float32)
    middle = (residual_in.astype(jnp.float32) + branch).astype(jnp.bfloat16)
    middle_wide = middle.astype(jnp.float32)
    row_scale = lax.rsqrt(jnp.mean(middle_wide * middle_wide, axis=1, keepdims=True) + 1e-06)
    normed = (middle_wide * row_scale * norm_gain.astype(jnp.float32)).astype(jnp.bfloat16)
    gate_pre = jnp.dot(
        normed,
        lax.all_gather(gate_weight, "sp", axis=0, tiled=True),
        preferred_element_type=jnp.float32,
    )
    up_pre = jnp.dot(
        normed,
        lax.all_gather(up_weight, "sp", axis=0, tiled=True),
        preferred_element_type=jnp.float32,
    )
    down_whole = lax.all_gather(down_weight, "sp", axis=0, tiled=True)
    hidden = (jax.nn.silu(gate_pre) * up_pre).astype(jnp.bfloat16)
    share = row_count // lax.axis_size("tp")
    channel_out = lax.psum_scatter(
        lax.dot_general(
            hidden, down_whole, (((1,), (1,)), ((), ())), preferred_element_type=jnp.float32
        ).astype(jnp.bfloat16),
        "tp",
        scatter_dimension=0,
        tiled=True,
    ).astype(jnp.float32)
    first_row = lax.axis_index("tp") * share
    own_rows = lax.dynamic_slice_in_dim(middle, first_row, share, 0)
    layer_rows = (own_rows.astype(jnp.float32) + channel_out).astype(jnp.bfloat16)
    return lax.all_gather(layer_rows, "tp", axis=0, tiled=True)


def solution(mesh):
    placed = (
        P("sp", None),
        P("tp", "sp"),
        P("tp", "sp"),
        P("tp", None),
        P("tp", None, None),
        P("tp", None, None),
        P("tp"),
        P("tp", "sp"),
        P("tp", None),
        P(),
        P("sp", "tp"),
        P("sp", "tp"),
        P("sp", "tp"),
    )
    return jax.shard_map(
        on_device, mesh=mesh, in_specs=placed, out_specs=P("sp", None), check_vma=False
    )
```
